32 devices in a mesh: sp: 8 (over z, core), tp: 4 (over y, x).
Axes of the slice: x: 2, y: 2, z: 4, core: 2. Of those that a mesh axis runs over, the one named last changes fastest.
Arguments:
- residual: bfloat16 [1024, 4096], P('sp', 'tp'), may hold values from -46 to 46
- query_small: bfloat16 [1024, 2048], P('sp', 'tp'), may hold values from -6 to 6
- key_narrow_group: bfloat16 [1024, 2048], P('sp', 'tp'), may hold values from -6 to 6
- query_large: bfloat16 [1024, 4096], P('sp', 'tp'), may hold values from -6 to 6
- key_large: bfloat16 [1024, 4096], P('sp', 'tp'), may hold values from -6 to 6
- values: bfloat16 [1024, 2, 2048], P('sp', None, 'tp'), may hold values from -6 to 6
- gates: bfloat16 [1024, 2, 2048], P('sp', None, 'tp'), may hold values from -6 to 6
- log_decay: float32 [1024, 2, 16], P('sp', None, 'tp'), may hold values from -0.65 to 0, as said below
- head_gain: float32 [2, 2048], P(None, 'tp'), may hold values from 0.1 to 1.9
- out_weight: bfloat16 [2, 2048, 4096], P(None, 'sp', 'tp'), may hold values from -0.09375 to 0.09375
- norm_gain: float32 [4096], P('tp'), may hold values from 0.1 to 1.9
- routes: int32 [1024, 2], P('sp'), may hold values from 0 to 7, all different within a row; in each aligned block of 128 rows (0 to 127, 128 to 255, ...) at most 64 rows name the same one
- route_weight: float32 [1024, 2], P('sp'), may hold values from 0.2 to 1
- expert_gate: bfloat16 [8, 4096, 2048], P('sp', None, 'tp'), may hold values from -0.09375 to 0.09375
- expert_up: bfloat16 [8, 4096, 2048], P('sp', None, 'tp'), may hold values from -0.09375 to 0.09375
- expert_down: bfloat16 [8, 2048, 4096], P('sp', None, 'tp'), may hold values from -0.5 to 0.5
Outputs:
- new_stream: bfloat16 [1024, 4096], P('sp', 'tp')
The draws below stay inside these ranges and needn't reach their ends.
Inputs may be any that keep to these rules, and one draw needn't show every extreme that they name: `routes`: each row names two different experts; in each aligned block of 128 rows no expert is named more than 64 times, a bound that some block reaches. `log_decay`: negative at every position.
All inputs are finite; a program needn't handle non-finite values.
Results may differ from the reference program's by a relative error of at most 0.019.
Values may be sent and summed in bfloat16 or wider, within the bound.
A program may use at most 64 MiB of HBM per device.

```python
import math
import jax
import jax.numpy as jnp
import numpy as np
from jax import lax

D = 4096
H = 16
DKA = 128
DKB = 256
DV = 128
FF = 2048
TOK_DEV = 128
TOKENS = 1024
EXPERTS = 8
CAP = 64
N_SP = 8


def draw_residual(key, part):
    keys = jax.random.split(key, 3)
    base = jnp.clip(jax.random.normal(keys[0], (TOKENS, D), jnp.float32), -5.0, 5.0)
    ramp = jnp.arange(D, dtype=jnp.float32) / D
    coarse_estimate = jax.random.uniform(keys[1], (1, D), jnp.float32, 0.5, 1.5)
    columns = 0.3 * jnp.power(10.0, ramp)
    row_scale = jnp.exp(jax.random.uniform(keys[2], (TOKENS, 1), jnp.float32, -0.7, 0.7))
    return (base * columns[None, :] * coarse_estimate * row_scale).astype(jnp.bfloat16)


def draw_log_decay(key, part):
    keys = jax.random.split(key, 7)
    choose = jax.random.uniform(keys[0], (1, 2, H), jnp.float32)
    slow_heads = choose < 0.5
    fast_rate = jnp.exp(-jax.random.uniform(keys[1], (1, 2, H), jnp.float32, 3.4, 4.1))
    slow_rate = jax.random.uniform(keys[2], (1, 2, H), jnp.float32, 0.1, 0.4) / TOKENS
    decay_speed = jnp.where(slow_heads, slow_rate, fast_rate)
    block_count = TOKENS // TOK_DEV
    multiplier_term = jnp.exp(jax.random.uniform(keys[3], (block_count, 1, 1), jnp.float32, -0.69, 0.69))
    multiplier_term = jnp.repeat(multiplier_term, TOK_DEV, axis=0)
    coarse_estimate = jax.random.uniform(keys[4], (TOKENS, 2, H), jnp.float32, 0.5, 1.5)
    spots = jax.random.randint(keys[5], (3,), 0, TOKENS)
    hit_marker = jnp.any(jnp.arange(TOKENS)[:, None] == spots[None, :], axis=1)
    kept_fraction = jax.random.uniform(keys[6], (TOKENS, 1, 1), jnp.float32, 0.6, 0.8)
    spike_amount = jnp.where(hit_marker[:, None, None], jnp.log(kept_fraction), 0.0)
    return (-decay_speed * multiplier_term * coarse_estimate + spike_amount).astype(jnp.float32)


def levels(stream_key, shape, cuts, smallest, high):
    def one(dim, parts):
        draws = jax.random.uniform(jax.random.fold_in(jax.random.fold_in(stream_key, 6), dim), (parts,), jnp.float32, smallest / len(cuts), high / len(cuts))
        return jnp.repeat(jnp.exp(draws), shape[dim] // parts).reshape((-1,) + (1,) * (len(shape) - dim - 1))

    level = one(*cuts[0])
    for cut in cuts[1:]:
        level = level * one(*cut)
    return level


def shared_out(rng, own, number, rows, count, top, reach, slope):
    order = jax.random.permutation(rng, count)
    packed, usual = portions_of(count, rows * top, reach, slope, True), portions_of(count, rows * top, reach, slope, False)
    places = jnp.arange(count)

    def named(lengths, rotation):
        used = int((lengths > 0).sum())
        fixed = max(1, used // 4)
        moved = fixed + (places - fixed + rotation * (used - fixed)) % max(1, count - fixed)
        return jnp.zeros((count,), jnp.int32).at[order[jnp.where(places < fixed, places, moved)]].set(jnp.asarray(lengths, jnp.int32))

    lengths = jnp.where(number % 4 == 0, named(packed, number // 4), named(usual, number - number // 4 - 1))
    mixed = jax.random.permutation(jax.random.fold_in(own, 3), count)
    donor, sink = mixed[0:count // 2 * 2:2], mixed[1:count // 2 * 2:2]
    margin = jnp.minimum(lengths[donor] - 1, reach - lengths[sink]) // 2
    margin = jnp.where((donor == order[0]) | (sink == order[0]) | (lengths[sink] == 0), 0, jnp.maximum(margin, 0))
    moved = jax.random.randint(jax.random.fold_in(own, 4), (count // 2,), 0, 1 << 20) % (margin + 1)
    lengths = lengths.at[donor].add(-moved).at[sink].add(moved)
    items = jnp.searchsorted(jnp.cumsum(lengths), jnp.arange(rows * top), side="right").astype(jnp.int32)
    listing = items.reshape(top, rows).T
    listing = listing[jax.random.permutation(jax.random.fold_in(own, 1), rows)]
    rotation = jax.random.randint(jax.random.fold_in(own, 2), (rows, 1), 0, top)
    return jnp.take_along_axis(listing, (jnp.arange(top)[None, :] + rotation) % top, axis=1)


def portions_of(amount, total, reach, skew, full):
    weights = [(1 << 20) // math.isqrt(grade ** skew) + 1 for grade in range(1, amount + 1)]
    largest = reach if full else min(reach, max(-(-total // amount), total * weights[0] // sum(weights)))
    least = 1 if total - largest >= amount - 1 else 0
    given, spare = [largest] + [least] * (amount - 1), total - largest - least * (amount - 1)
    while spare > 0:
        candidates = [i for i in range(1, amount) if given[i] < largest] or [i for i in range(1, amount) if given[i] < reach]
        whole, left = sum([weights[i] for i in candidates]), spare
        for i in candidates:
            extra = min(reach - given[i], max(1, left * weights[i] // whole), spare)
            given[i] = given[i] + extra
            spare = spare - extra
    return np.array(given)


def scatter_about(own_key, dims, scale, most, cuts=(), held_as=jnp.bfloat16):
    result = jax.random.normal(own_key, dims, jnp.float32) * scale
    if len(cuts) > 0:
        result = levels(own_key, dims, cuts, -0.22, 0.18) * result
    return jnp.clip(result, min=-most, max=most).astype(held_as)


def setup_inputs(seed: int = 0) -> dict:
    key_of = jax.random.split(jax.random.key(seed), 17)
    residual = draw_residual(jax.random.fold_in(key_of[16], 71), 0)
    query_small = scatter_about(key_of[1], (TOKENS, H * DKA), 1.0, 6.0, ((0, 8), (1, 4)))
    key_narrow_group = scatter_about(key_of[2], (TOKENS, H * DKA), 1.0, 6.0, ((0, 8), (1, 4)))
    query_large = scatter_about(key_of[3], (TOKENS, H * DKB), 1.0, 6.0, ((0, 8), (1, 4)))
    key_large = scatter_about(key_of[4], (TOKENS, H * DKB), 1.0, 6.0, ((0, 8), (1, 4)))
    values = scatter_about(key_of[5], (TOKENS, 2, H * DV), 1.0, 6.0, ((0, 8), (2, 4)))
    gates = scatter_about(key_of[6], (TOKENS, 2, H * DV), 1.0, 6.0, ((0, 8), (2, 4)))
    log_decay = draw_log_decay(jax.random.fold_in(key_of[16], 71), 0)
    head_gain = jnp.clip(1.0 + 0.18 * jax.random.normal(key_of[8], (2, H * DV), jnp.float32), 0.1, 1.9)
    out_weight = scatter_about(key_of[9], (2, H * DV, D), (2 * H * DV) ** -0.5, 0.09375, ((1, 8), (2, 4)))
    norm_gain = jnp.clip(1.0 + 0.18 * jax.random.normal(key_of[10], (D,), jnp.float32), 0.1, 1.9)
    routes_keys = jax.random.split(jax.random.fold_in(key_of[11], 1), TOKENS // TOK_DEV)
    routes_turns = jax.random.permutation(jax.random.fold_in(key_of[11], 3), TOKENS // TOK_DEV)
    routes = jax.vmap(lambda own, number: shared_out(jax.random.fold_in(key_of[11], 2), own, number, TOK_DEV, EXPERTS, 2, CAP, 2))(routes_keys, routes_turns).reshape((TOKENS, 2))
    route_weight = jnp.clip(0.2 + 0.8 * jax.random.uniform(key_of[12], (TOKENS, 2), jnp.float32) ** levels(key_of[12], (TOKENS, 2), ((0, 8),), -0.2, 0.2), 0.2, 1.0)
    expert_gate = scatter_about(key_of[13], (EXPERTS, D, FF), D ** -0.5, 0.09375, ((0, 8), (2, 4)))
    expert_up = scatter_about(key_of[14], (EXPERTS, D, FF), D ** -0.5, 0.09375, ((0, 8), (2, 4)))
    expert_down = scatter_about(key_of[15], (EXPERTS, FF, D), (FF // 16) ** -0.5, 0.5, ((0, 8), (2, 4)))
    return {"residual": residual, "query_small": query_small, "key_narrow_group": key_narrow_group, "query_large": query_large, "key_large": key_large, "values": values, "gates": gates, "log_decay": log_decay, "head_gain": head_gain, "out_weight": out_weight, "norm_gain": norm_gain, "routes": routes, "route_weight": route_weight, "expert_gate": expert_gate, "expert_up": expert_up, "expert_down": expert_down}


EPS = 1e-06
THETA = 10000.0

def rotate(block, positions):
    half_dim = block.shape[-1] // 2
    inverse = jnp.power(THETA, -jnp.arange(half_dim, dtype=jnp.float32) * 2.0 / block.shape[-1])
    angles = positions[:, None, None] * inverse
    cosine_val, sine_val = (jnp.cos(angles), jnp.sin(angles))
    lower_half, upper_half = (block[..., :half_dim], block[..., half_dim:])
    return jnp.concatenate([lower_half * cosine_val - upper_half * sine_val, upper_half * cosine_val + lower_half * sine_val], axis=-1)

def block_terms(rot_queries, rot_keys, value_heads, rates):
    count = rates.shape[0]
    decay_sum = jnp.cumsum(rates, axis=0)
    by_head = decay_sum.T
    causal = (jnp.arange(count)[:, None] >= jnp.arange(count)[None, :])[None]
    spread = by_head[:, :, None] - by_head[:, None, :]
    weight = jnp.where(causal, jnp.exp(jnp.where(causal, spread, 0.0)), 0.0)
    scores = jnp.einsum('ihd,jhd->hij', rot_queries.astype(jnp.float32), rot_keys.astype(jnp.float32))
    weighted = (scores * weight).astype(jnp.bfloat16)
    within = jnp.einsum('hij,jhv->ihv', weighted.astype(jnp.float32), value_heads.astype(jnp.float32))
    block_end = decay_sum[-1]
    carried = (rot_keys.astype(jnp.float32) * jnp.exp(block_end[None, :] - decay_sum)[:, :, None]).astype(jnp.bfloat16)
    update = jnp.einsum('jhd,jhv->hdv', carried.astype(jnp.float32), value_heads.astype(jnp.float32))
    return (within, decay_sum, jnp.exp(block_end), update)

def final_result(rot_queries, decay_sum, within, state_in, gate_part, gain_part):
    cross_part = jnp.einsum('ihd,hdv->ihv', rot_queries.astype(jnp.float32), state_in, precision=lax.Precision.HIGHEST) * jnp.exp(decay_sum)[:, :, None]
    retained = within + cross_part
    scaled = retained * lax.rsqrt(lax.optimization_barrier(jnp.mean(retained * retained, axis=-1, keepdims=True)) + EPS)
    count, head_count, value_size = retained.shape
    gated = jax.nn.silu(gate_part.astype(jnp.float32)).reshape(count, head_count, value_size)
    return (scaled * gain_part.reshape(head_count, value_size) * gated).reshape(count, -1).astype(jnp.bfloat16)

def group_out(queries, keys_in, value_part, gate_part, rates, gain_part, key_size):
    length = queries.shape[0]
    head_count = rates.shape[1]
    value_size = value_part.shape[1] // head_count
    positions = jnp.arange(length, dtype=jnp.float32)
    rot_queries = rotate(queries.astype(jnp.float32).reshape(length, head_count, key_size), positions).astype(jnp.bfloat16)
    rot_keys = (rotate(keys_in.astype(jnp.float32).reshape(length, head_count, key_size), positions) * key_size ** (-0.5)).astype(jnp.bfloat16)
    value_heads = value_part.reshape(length, head_count, value_size)
    block_count = length // TOK_DEV

    def split_blocks(array):
        return array.reshape((block_count, TOK_DEV) + array.shape[1:])

    def advance(state, inputs):
        block_q, block_k, block_v, block_rates, block_gate = inputs
        within, decay_sum, fall, update = block_terms(block_q, block_k, block_v, block_rates)
        output = final_result(block_q, decay_sum, within, state, block_gate, gain_part)
        return (fall[:, None, None] * state + update, output)
    start_state = jnp.zeros((head_count, key_size, value_size), jnp.float32)
    _, outputs = lax.scan(advance, start_state, (split_blocks(rot_queries), split_blocks(rot_keys), split_blocks(value_heads), split_blocks(rates), split_blocks(gate_part)))
    return outputs.reshape(length, head_count * value_size)

def reference(residual, query_small, key_narrow_group, query_large, key_large, values, gates, log_decay, head_gain, out_weight, norm_gain, routes, route_weight, expert_gate, expert_up, expert_down):
    out_small = group_out(query_small, key_narrow_group, values[:, 0], gates[:, 0], log_decay[:, 0], head_gain[0], DKA)
    out_large = group_out(query_large, key_large, values[:, 1], gates[:, 1], log_decay[:, 1], head_gain[1], DKB)
    mixed = (jnp.dot(out_small, out_weight[0], preferred_element_type=jnp.float32) + jnp.dot(out_large, out_weight[1], preferred_element_type=jnp.float32)).astype(jnp.bfloat16)
    stream = residual.astype(jnp.float32) + mixed.astype(jnp.float32)
    normed = (stream * lax.rsqrt(lax.optimization_barrier(jnp.mean(stream * stream, axis=-1, keepdims=True)) + EPS) * norm_gain[None, :]).astype(jnp.bfloat16)
    experts = N_SP
    capacity = 4 * TOK_DEV // experts
    one_hot = (routes[:, :, None] == jnp.arange(experts, dtype=jnp.int32)[None, None, :]).astype(jnp.int32)
    one_hot = one_hot.reshape(N_SP, 2 * TOK_DEV, experts)
    before = jnp.cumsum(one_hot, axis=1) - one_hot
    slot_index = lax.optimization_barrier(jnp.sum(before * one_hot, axis=2)).reshape(TOKENS, 2)
    block_index = (jnp.arange(TOKENS, dtype=jnp.int32) // TOK_DEV).astype(jnp.int32)
    row_slot = (block_index[:, None] * capacity + slot_index).astype(jnp.int32)
    buffer = jnp.zeros((experts, N_SP * capacity, D), jnp.bfloat16)
    buffer = buffer.at[routes, row_slot].set(jnp.broadcast_to(normed[:, None, :], (TOKENS, 2, D)))

    def apply_expert(operands):
        rows_in, w_gate, w_up, w_down = operands
        gate_part = jnp.dot(rows_in, w_gate, preferred_element_type=jnp.float32)
        up_part = jnp.dot(rows_in, w_up, preferred_element_type=jnp.float32)
        hidden = (jax.nn.silu(gate_part) * up_part).astype(jnp.bfloat16)
        return jnp.dot(hidden, w_down, preferred_element_type=jnp.float32).astype(jnp.bfloat16)
    results = lax.map(apply_expert, (buffer, expert_gate, expert_up, expert_down))
    first_pick = results[routes[:, 0], row_slot[:, 0]].astype(jnp.float32)
    second_pick = results[routes[:, 1], row_slot[:, 1]].astype(jnp.float32)
    routed = route_weight[:, 0:1] * first_pick + route_weight[:, 1:2] * second_pick
    return (stream + routed).astype(jnp.bfloat16)
```

```python
import jax
import jax.numpy as jnp
from jax import lax
from jax.experimental import pallas as pl
from jax.experimental.pallas import tpu as pltpu
from jax.sharding import PartitionSpec as P

MESH = pl.DeviceIdType.MESH


EPS = 1e-06
THETA = 10000.0


def greet(axes):
    barrier = pltpu.get_barrier_semaphore()
    total = 0
    for axis in axes:
        count, me = lax.axis_size(axis), lax.axis_index(axis)

        def signal(k, _, axis=axis, count=count, me=me):
            pl.semaphore_signal(
                barrier, inc=1, device_id={axis: (me + k) % count}, device_id_type=MESH
            )
            return 0

        lax.fori_loop(1, count, signal, 0)
        total += count - 1
    pl.semaphore_wait(barrier, total)


def remote(source, target, send_sem, recv_sem, axis, index):
    return pltpu.make_async_remote_copy(
        src_ref=source,
        dst_ref=target,
        send_sem=send_sem,
        recv_sem=recv_sem,
        device_id={axis: index},
        device_id_type=MESH,
    )


def chain_kernel(update_ref, fall_ref, out_ref, held, outgoing, send_sem, recv_sem):
    count, me = lax.axis_size("sp"), lax.axis_index("sp")
    pieces = update_ref.shape[0]
    right, left = (me + 1) % count, (me + count - 1) % count
    barrier = pltpu.get_barrier_semaphore()
    for neighbour in (left, right):
        pl.semaphore_signal(barrier, inc=1, device_id={"sp": neighbour}, device_id_type=MESH)
    pl.semaphore_wait(barrier, 2)

    def hop(c):
        return remote(
            outgoing.at[c], held.at[c], send_sem.at[c], recv_sem.at[c], "sp", right
        )

    def step(c, _):
        @pl.when(me == 0)
        def _():
            held[c] = jnp.zeros(held.shape[1:], held.dtype)

        @pl.when(me > 0)
        def _():
            hop(c).wait_recv()

        @pl.when(me < count - 1)
        def _():
            outgoing[c] = (fall_ref[c] * held[c].astype(jnp.float32) + update_ref[c]).astype(
                outgoing.dtype
            )
            hop(c).start()

        out_ref[c] = held[c]
        return 0

    lax.fori_loop(0, pieces, step, 0)

    @pl.when(me < count - 1)
    def _():
        def finish(c, _):
            hop(c).wait_send()
            return 0

        lax.fori_loop(0, pieces, finish, 0)


def entering_states(update, fall):
    pieces, rows, columns = update.shape
    return pl.pallas_call(
        chain_kernel,
        out_shape=jax.ShapeDtypeStruct(update.shape, jnp.bfloat16),
        in_specs=[pl.BlockSpec(memory_space=pltpu.VMEM)] * 2,
        out_specs=pl.BlockSpec(memory_space=pltpu.VMEM),
        scratch_shapes=[
            pltpu.VMEM((pieces, rows, columns), jnp.bfloat16),
            pltpu.VMEM((pieces, rows, columns), jnp.bfloat16),
            pltpu.SemaphoreType.DMA((pieces,)),
            pltpu.SemaphoreType.DMA((pieces,)),
        ],
        compiler_params=pltpu.CompilerParams(collective_id=0, has_side_effects=True),
    )(update, fall)


def gather_kernel(part_ref, out_ref, held, send_sem, recv_sem):
    count, me = lax.axis_size("tp"), lax.axis_index("tp")
    width = part_ref.shape[2]
    greet(("tp",))

    def place(index):
        return held.at[:, :, pl.ds(pl.multiple_of(index * width, width), width)]

    def start(k, _):
        remote(part_ref, place(me), send_sem.at[k], recv_sem.at[me], "tp", (me + k) % count).start()
        return 0

    lax.fori_loop(1, count, start, 0)
    held[:, :, pl.ds(pl.multiple_of(me * width, width), width)] = part_ref[...]

    def finish(k, _):
        other = (me + k) % count
        remote(part_ref, place(other), send_sem.at[k], recv_sem.at[other], "tp", other).wait()
        return 0

    lax.fori_loop(1, count, finish, 0)
    out_ref[...] = held[...]


def gather_heads(part, count):
    whole = part.shape[:2] + (part.shape[2] * count,)
    return pl.pallas_call(
        gather_kernel,
        out_shape=jax.ShapeDtypeStruct(whole, part.dtype),
        in_specs=[pl.BlockSpec(memory_space=pltpu.VMEM)],
        out_specs=pl.BlockSpec(memory_space=pltpu.VMEM),
        scratch_shapes=[
            pltpu.VMEM(whole, part.dtype),
            pltpu.SemaphoreType.DMA((count,)),
            pltpu.SemaphoreType.DMA((count,)),
        ],
        compiler_params=pltpu.CompilerParams(collective_id=1, has_side_effects=True),
    )(part)


def experts_kernel(
    stream_ref,
    gain_ref,
    select_ref,
    gate_hbm,
    up_hbm,
    down_hbm,
    out_ref,
    w_gate,
    w_up,
    w_down,
    squares,
    outgoing,
    arrived,
    hidden,
    result,
    returned,
    acc_a,
    acc_b,
    acc_c,
    load_sem,
    sq_send,
    sq_recv,
    disp_send,
    disp_recv,
    fwd_send,
    fwd_recv,
    fwd_relay_send,
    fwd_relay_recv,
    hid_send,
    hid_recv,
    hid_relay_send,
    hid_relay_recv,
    ret_send,
    ret_recv,
):
    n_sp, n_tp = lax.axis_size("sp"), lax.axis_size("tp")
    s, t = lax.axis_index("sp"), lax.axis_index("tp")
    per_group = n_sp // GROUPS
    across, down = grid_of(n_tp)
    x, y = t % across, t // across
    cap = outgoing.shape[0] // n_sp
    cols = stream_ref.shape[1]
    units = w_gate.shape[1]
    loads = [
        pltpu.make_async_copy(source.at[0], target, load_sem.at[i])
        for i, (source, target) in enumerate(
            ((gate_hbm, w_gate), (up_hbm, w_up), (down_hbm, w_down))
        )
    ]
    for load in loads:
        load.start()
    greet(("sp", "tp"))

    def rows_of(p):
        return pl.ds(pl.multiple_of(p * cap, cap), cap)

    def group_base(g):
        return ((s // per_group + g) % GROUPS) * per_group

    def group_rows(g, part=None):
        size = per_group * cap
        start = pl.multiple_of(group_base(g) * cap, size)
        if part is None:
            return pl.ds(start, size)
        return pl.ds(pl.multiple_of(start + part * (size // 2), size // 2), size // 2)

    lines = (
        [y * across + (x + k) % across for k in range(1, across)],
        [((y + k) % down) * across + x for k in range(1, down)],
    )
    direct = lines[0] + lines[1]

    stream = stream_ref[...]
    own = jnp.sum(stream * stream, axis=1, keepdims=True)
    squares[t] = jnp.broadcast_to(own, squares.shape[1:])

    def square_copy(k, source):
        block, other = squares.at[source], (t + k) % n_tp
        return remote(block, block, sq_send.at[k], sq_recv.at[source], "tp", other)

    def square_start(k, _):
        square_copy(k, t).start()
        return 0

    def square_wait(k, _):
        square_copy(k, (t + k) % n_tp).wait()
        return 0

    lax.fori_loop(1, n_tp, square_start, 0)
    lax.fori_loop(1, n_tp, square_wait, 0)
    total = squares[0]
    for p in range(1, n_tp):
        total = total + squares[p]
    scale = lax.rsqrt(total[:, 0:1] / (cols * n_tp) + EPS)
    normed = (stream_ref[...] * scale * gain_ref[...]).astype(jnp.bfloat16)
    outgoing[...] = jnp.dot(
        select_ref[...], normed, preferred_element_type=jnp.float32
    ).astype(jnp.bfloat16)

    def dispatch(p, q):
        return remote(
            outgoing.at[rows_of(p)],
            arrived.at[t, rows_of(q)],
            disp_send.at[p],
            disp_recv.at[q],
            "sp",
            p,
        )

    def members(g, action):
        def body(j, _):
            action(group_base(g) + (s + j) % per_group)
            return 0

        lax.fori_loop(0, per_group, body, 0)

    def others(g, action):
        def guarded(p):
            @pl.when(p != s)
            def _():
                action(p)

        members(g, guarded)

    for g in range(GROUPS):
        others(g, lambda p: dispatch(p, s).start())
    arrived[t, rows_of(s)] = outgoing[rows_of(s)]

    def straight(buffer, sems, g, i, source, rows):
        block = buffer.at[source, rows]
        return remote(block, block, sems[0].at[g, i], sems[1].at[g, source], "tp", direct[i])

    def relayed(buffer, sems, g, part, i, source, target):
        block = buffer.at[source, group_rows(g, part)]
        return remote(
            block, block, sems[2].at[g, part, i], sems[3].at[g, source, part], "tp", target
        )

    def relay(buffer, sems, g):
        for part in range(2):
            for k, source in enumerate(lines[part]):
                i = k if part == 0 else len(lines[0]) + k
                straight(buffer, sems, g, i, source, group_rows(g)).wait_recv()
                for j, target in enumerate(lines[1 - part]):
                    relayed(
                        buffer, sems, g, part, k * len(lines[1 - part]) + j, source, target
                    ).start()

    def place_of(k):
        return ((y + k // across) % down) * across + (x + k % across) % across

    def wait_relayed(buffer, sems, g, k):
        @pl.when((k // across) * (k % across) > 0)
        def _():
            source = place_of(k)
            for part in range(2):
                relayed(buffer, sems, g, part, 0, source, source).wait_recv()

    def finish_sends(buffer, sems, g):
        for i in range(len(direct)):
            straight(buffer, sems, g, i, t, group_rows(g)).wait_send()
        for part in range(2):
            for i in range(len(lines[0]) * len(lines[1])):
                relayed(buffer, sems, g, part, i, t, direct[0]).wait_send()

    arrived_sems = (fwd_send, fwd_recv, fwd_relay_send, fwd_relay_recv)
    hidden_sems = (hid_send, hid_recv, hid_relay_send, hid_relay_recv)

    def forward(g):
        def block(p):
            @pl.when(p != s)
            def _():
                dispatch(p, p).wait_recv()

            for i in range(len(direct)):
                straight(arrived, arrived_sems, g, i, t, rows_of(p)).start()

        members(g, block)

    def through_units(g):
        acc_a[...] = jnp.zeros_like(acc_a)
        acc_b[...] = jnp.zeros_like(acc_b)

        def body(k, _):
            wait_relayed(arrived, arrived_sems, g, k)
            p = place_of(k)
            part = pl.ds(pl.multiple_of(p * cols, cols), cols)
            rows = arrived[p, group_rows(g)]
            acc_a[...] += jnp.dot(rows, w_gate[part, :], preferred_element_type=jnp.float32)
            acc_b[...] += jnp.dot(rows, w_up[part, :], preferred_element_type=jnp.float32)
            return 0

        lax.fori_loop(0, n_tp, body, 0)
        hidden[t, group_rows(g)] = (jax.nn.silu(acc_a[...]) * acc_b[...]).astype(jnp.bfloat16)
        for i in range(len(direct)):
            straight(hidden, hidden_sems, g, i, t, group_rows(g)).start()

    def give_back(p, q):
        return remote(
            result.at[rows_of(p)], returned.at[rows_of(q)], ret_send.at[p], ret_recv.at[q], "sp", p
        )

    def through_down(g):
        acc_c[...] = jnp.zeros_like(acc_c)

        def body(k, _):
            wait_relayed(hidden, hidden_sems, g, k)
            p = place_of(k)
            part = pl.ds(pl.multiple_of(p * units, units), units)
            acc_c[...] += jnp.dot(
                hidden[p, group_rows(g)], w_down[part, :], preferred_element_type=jnp.float32
            )
            return 0

        lax.fori_loop(0, n_tp, body, 0)
        result[group_rows(g)] = acc_c[...].astype(jnp.bfloat16)
        others(g, lambda p: give_back(p, s).start())

    for step in range(GROUPS + 4):
        for late, action in enumerate(
            (
                forward,
                lambda g: relay(arrived, arrived_sems, g),
                through_units,
                lambda g: relay(hidden, hidden_sems, g),
                through_down,
            )
        ):
            if 0 <= step - late < GROUPS:
                if late == 2 and step == 2:
                    for load in loads:
                        load.wait()
                action(step - late)
    returned[rows_of(s)] = result[rows_of(s)]
    for g in range(GROUPS):
        others(g, lambda p: give_back(p, p).wait_recv())
    out_ref[...] = returned[...]
    for g in range(GROUPS):
        others(g, lambda p: dispatch(p, s).wait_send())
        others(g, lambda p: give_back(p, s).wait_send())
        finish_sends(arrived, arrived_sems, g)
        finish_sends(hidden, hidden_sems, g)


GROUPS = 4


def grid_of(count):
    across = max(k for k in range(1, count + 1) if count % k == 0 and k * k <= count)
    return across, count // across


def through_experts(stream, gain, select, w_gate, w_up, w_down, n_sp, n_tp):
    count, cols = stream.shape
    slots = select.shape[0]
    width, units = w_gate.shape[1:]
    bf16, f32 = jnp.bfloat16, jnp.float32
    dma = pltpu.SemaphoreType.DMA
    across, down = grid_of(n_tp)
    straights, relays = across + down - 2, (across - 1) * (down - 1)
    vmem = pl.BlockSpec(memory_space=pltpu.VMEM)
    hbm = pl.BlockSpec(memory_space=pl.ANY)
    return pl.pallas_call(
        experts_kernel,
        out_shape=jax.ShapeDtypeStruct((slots, cols), bf16),
        in_specs=[vmem] * 3 + [hbm] * 3,
        out_specs=vmem,
        scratch_shapes=[
            pltpu.VMEM((width, units), bf16),
            pltpu.VMEM((width, units), bf16),
            pltpu.VMEM(w_down.shape[1:], bf16),
            pltpu.VMEM((n_tp, count, 128), f32),
            pltpu.VMEM((slots, cols), bf16),
            pltpu.VMEM((n_tp, slots, cols), bf16),
            pltpu.VMEM((n_tp, slots, units), bf16),
            pltpu.VMEM((slots, cols), bf16),
            pltpu.VMEM((slots, cols), bf16),
            pltpu.VMEM((slots // GROUPS, units), f32),
            pltpu.VMEM((slots // GROUPS, units), f32),
            pltpu.VMEM((slots // GROUPS, cols), f32),
            dma((3,)),
            dma((n_tp,)),
            dma((n_tp,)),
            dma((n_sp,)),
            dma((n_sp,)),
            dma((GROUPS, straights)),
            dma((GROUPS, n_tp)),
            dma((GROUPS, 2, relays)),
            dma((GROUPS, n_tp, 2)),
            dma((GROUPS, straights)),
            dma((GROUPS, n_tp)),
            dma((GROUPS, 2, relays)),
            dma((GROUPS, n_tp, 2)),
            dma((n_sp,)),
            dma((n_sp,)),
        ],
        compiler_params=pltpu.CompilerParams(
            collective_id=2, has_side_effects=True, vmem_limit_bytes=50 * 2**20
        ),
    )(stream, gain, select, w_gate, w_up, w_down)


def rotate(block, positions):
    half_dim = block.shape[-1] // 2
    inverse = jnp.power(THETA, -jnp.arange(half_dim, dtype=jnp.float32) * 2.0 / block.shape[-1])
    angles = positions[:, None, None] * inverse
    cosine_val, sine_val = (jnp.cos(angles), jnp.sin(angles))
    lower_half, upper_half = (block[..., :half_dim], block[..., half_dim:])
    return jnp.concatenate(
        [
            lower_half * cosine_val - upper_half * sine_val,
            upper_half * cosine_val + lower_half * sine_val,
        ],
        axis=-1,
    )


def block_terms(rot_queries, rot_keys, value_heads, rates):
    count = rates.shape[0]
    decay_sum = jnp.cumsum(rates, axis=0)
    by_head = decay_sum.T
    causal = (jnp.arange(count)[:, None] >= jnp.arange(count)[None, :])[None]
    spread = by_head[:, :, None] - by_head[:, None, :]
    weight = jnp.where(causal, jnp.exp(jnp.where(causal, spread, 0.0)), 0.0)
    scores = jnp.einsum("ihd,jhd->hij", rot_queries, rot_keys, preferred_element_type=jnp.float32)
    weighted = (scores * weight).astype(jnp.bfloat16)
    within = jnp.einsum("hij,jhv->ihv", weighted, value_heads, preferred_element_type=jnp.float32)
    block_end = decay_sum[-1]
    carried = (
        rot_keys.astype(jnp.float32) * jnp.exp(block_end[None, :] - decay_sum)[:, :, None]
    ).astype(jnp.bfloat16)
    update = jnp.einsum("jhd,jhv->hdv", carried, value_heads, preferred_element_type=jnp.float32)
    return (within, decay_sum, jnp.exp(block_end), update)


def final_result(rot_queries, decay_sum, within, state_in, gate_part, gain_part):
    cross_part = (
        jnp.einsum(
            "ihd,hdv->ihv",
            rot_queries,
            state_in,
            preferred_element_type=jnp.float32,
        )
        * jnp.exp(decay_sum)[:, :, None]
    )
    retained = within + cross_part
    scaled = retained * lax.rsqrt(jnp.mean(retained * retained, axis=-1, keepdims=True) + EPS)
    count, head_count, value_size = retained.shape
    gated = jax.nn.silu(gate_part.astype(jnp.float32)).reshape(count, head_count, value_size)
    return (
        (scaled * gain_part.reshape(head_count, value_size) * gated)
        .reshape(count, -1)
        .astype(jnp.bfloat16)
    )


def prepare(queries, keys_in, value_part, positions, head_count):
    row_count = queries.shape[0]
    key_size = queries.shape[1] // head_count
    rot_queries = rotate(
        queries.astype(jnp.float32).reshape(row_count, head_count, key_size), positions
    ).astype(jnp.bfloat16)
    rot_keys = (
        rotate(keys_in.astype(jnp.float32).reshape(row_count, head_count, key_size), positions)
        * key_size ** (-0.5)
    ).astype(jnp.bfloat16)
    value_heads = value_part.reshape(row_count, head_count, value_part.shape[1] // head_count)
    return (rot_queries, rot_keys, value_heads)


def spread_weight(block):
    count, me = lax.axis_size("sp"), lax.axis_index("sp")
    chips = count // 2
    mine = [(me, block)]
    for k in range(1, chips):
        pairs = [(s, (s + 2 * k) % count) for s in range(count)]
        mine.append(((me - 2 * k) % count, lax.ppermute(block, "sp", pairs)))
    swap = [(s, s ^ 1) for s in range(count)]
    other = [(source ^ 1, lax.ppermute(got, "sp", swap)) for source, got in mine]
    return mine + other


def per_device(
    residual,
    query_small,
    key_narrow_group,
    query_large,
    key_large,
    values,
    gates,
    log_decay,
    head_gain,
    out_weight,
    norm_gain,
    routes,
    route_weight,
    expert_gate,
    expert_up,
    expert_down,
):
    row_count = residual.shape[0]
    head_count = log_decay.shape[2]
    weight_blocks = spread_weight(out_weight)
    positions = (lax.axis_index("sp") * row_count + jnp.arange(row_count, dtype=jnp.int32)).astype(
        jnp.float32
    )
    query_a, key_a, value_a = prepare(
        query_small, key_narrow_group, values[:, 0], positions, head_count
    )
    query_b, key_b, value_b = prepare(query_large, key_large, values[:, 1], positions, head_count)
    within_a, decay_sum_a, fall_a, update_a = block_terms(query_a, key_a, value_a, log_decay[:, 0])
    within_b, decay_sum_b, fall_b, update_b = block_terms(query_b, key_b, value_b, log_decay[:, 1])

    n_sp, n_tp = lax.axis_size("sp"), lax.axis_size("tp")
    value_size = update_a.shape[2]
    piece = update_a.shape[1]
    parts = update_b.shape[1] // piece
    update = jnp.concatenate([update_a, update_b.reshape(-1, piece, value_size)], axis=0)
    fall = jnp.concatenate([fall_a, jnp.repeat(fall_b, parts)])
    fall = jnp.broadcast_to(fall[:, None, None], (fall.shape[0], 1, value_size))
    entering = entering_states(update, fall)
    state_a = entering[:head_count]
    state_b = entering[head_count:].reshape(update_b.shape)
    output_a = final_result(query_a, decay_sum_a, within_a, state_a, gates[:, 0], head_gain[0])
    output_b = final_result(query_b, decay_sum_b, within_b, state_b, gates[:, 1], head_gain[1])
    gathered = gather_heads(jnp.stack([output_a, output_b], axis=0), n_tp)
    held = out_weight.shape[1]
    me = lax.axis_index("sp")
    total = jnp.zeros((row_count, out_weight.shape[2]), jnp.float32)
    for source, block in weight_blocks:
        for g in range(2):
            part = lax.dynamic_slice_in_dim(gathered[g], source * held, held, axis=1)
            total = total + jnp.dot(part, block[g], preferred_element_type=jnp.float32)
    mixed = total.astype(jnp.bfloat16)
    stream = residual.astype(jnp.float32) + mixed.astype(jnp.float32)
    experts = lax.axis_size("sp")
    capacity = 4 * row_count // experts
    one_hot = (routes[:, :, None] == jnp.arange(experts, dtype=jnp.int32)[None, None, :]).astype(
        jnp.int32
    )
    one_hot = one_hot.reshape(2 * row_count, experts)
    before = jnp.cumsum(one_hot, axis=0) - one_hot
    slot_index = jnp.sum(before * one_hot, axis=1).reshape(row_count, 2)
    target = routes * capacity + slot_index
    slot_ids = jnp.arange(experts * capacity, dtype=jnp.int32)
    choose = target[:, :, None] == slot_ids[None, None, :]
    select = jnp.sum(choose.astype(jnp.int32), axis=1).astype(jnp.bfloat16).T
    returned = through_experts(
        stream, norm_gain[None, :], select, expert_gate, expert_up, expert_down, n_sp, n_tp
    )
    first_pick = jnp.dot(
        choose[:, 0].astype(jnp.bfloat16), returned, preferred_element_type=jnp.float32
    )
    second_pick = jnp.dot(
        choose[:, 1].astype(jnp.bfloat16), returned, preferred_element_type=jnp.float32
    )
    routed = route_weight[:, 0:1] * first_pick + route_weight[:, 1:2] * second_pick
    return (stream + routed).astype(jnp.bfloat16)


def solution(mesh):
    placed = (
        P("sp", "tp"),
        P("sp", "tp"),
        P("sp", "tp"),
        P("sp", "tp"),
        P("sp", "tp"),
        P("sp", None, "tp"),
        P("sp", None, "tp"),
        P("sp", None, "tp"),
        P(None, "tp"),
        P(None, "sp", "tp"),
        P("tp"),
        P("sp", None),
        P("sp", None),
        P("sp", None, "tp"),
        P("sp", None, "tp"),
        P("sp", None, "tp"),
    )
    return jax.shard_map(
        per_device, mesh=mesh, in_specs=placed, out_specs=P("sp", "tp"), check_vma=False
    )
```

```python
import jax
import jax.numpy as jnp
from jax import lax
from jax.experimental import pallas as pl
from jax.experimental.pallas import tpu as pltpu
from jax.sharding import PartitionSpec as P

MESH = pl.DeviceIdType.MESH


EPS = 1e-06
THETA = 10000.0


def greet(axes):
    barrier = pltpu.get_barrier_semaphore()
    total = 0
    for axis in axes:
        count, me = lax.axis_size(axis), lax.axis_index(axis)

        def signal(k, _, axis=axis, count=count, me=me):
            pl.semaphore_signal(
                barrier, inc=1, device_id={axis: (me + k) % count}, device_id_type=MESH
            )
            return 0

        lax.fori_loop(1, count, signal, 0)
        total += count - 1
    pl.semaphore_wait(barrier, total)


def remote(source, target, send_sem, recv_sem, axis, index):
    return pltpu.make_async_remote_copy(
        src_ref=source,
        dst_ref=target,
        send_sem=send_sem,
        recv_sem=recv_sem,
        device_id={axis: index},
        device_id_type=MESH,
    )


GROUPS = 4


def grid_of(count):
    across = max(k for k in range(1, count + 1) if count % k == 0 and k * k <= count)
    return across, count // across


def group_order():
    middle = (GROUPS - 1) / 2
    return sorted(range(GROUPS), key=lambda g: (abs(g - middle), g))


def turned(block, cosine, sine):
    half = block.shape[1] // 2
    if half % 128:
        swapped = pltpu.roll(block, half, axis=1)
    else:
        swapped = jnp.concatenate([block[:, half:], block[:, :half]], axis=1)
    return block * cosine + swapped * sine


def layer_kernel(
    residual_ref,
    query_a_ref,
    key_a_ref,
    query_b_ref,
    key_b_ref,
    values_ref,
    gates_ref,
    cos_a_ref,
    sin_a_ref,
    cos_b_ref,
    sin_b_ref,
    cumul_ref,
    cumul_rows_ref,
    head_gain_ref,
    gain_ref,
    target_ref,
    weight_hbm,
    gate_hbm,
    up_hbm,
    down_hbm,
    out_ref,
    stream_ref,
    rot_queries_a,
    rot_queries_b,
    within,
    update,
    fall,
    held,
    departing,
    heads,
    w_out,
    mix,
    w_gate,
    w_up,
    w_down,
    squares,
    outgoing,
    arrived,
    hidden,
    result,
    returned,
    acc_a,
    acc_b,
    acc_c,
    load_sem,
    chain_send,
    chain_recv,
    heads_send,
    heads_recv,
    w_line_send,
    w_pair_send,
    w_recv,
    sq_send,
    sq_recv,
    disp_send,
    disp_recv,
    fwd_send,
    fwd_recv,
    fwd_relay_send,
    fwd_relay_recv,
    hid_send,
    hid_recv,
    hid_relay_send,
    hid_relay_recv,
    ret_send,
    ret_recv,
):
    n_sp, n_tp = lax.axis_size("sp"), lax.axis_size("tp")
    s, t = lax.axis_index("sp"), lax.axis_index("tp")
    bf16, f32 = jnp.bfloat16, jnp.float32
    per_group = n_sp // GROUPS
    order = group_order()
    across, down = grid_of(n_tp)
    x, y = t % across, t // across
    cap = outgoing.shape[0] // n_sp
    cols = stream_ref.shape[1]
    units = w_gate.shape[1]
    count = stream_ref.shape[0]
    chips = n_sp // 2
    z, core = s // 2, s % 2
    loads = [
        pltpu.make_async_copy(source.at[0], target, load_sem.at[i])
        for i, (source, target) in enumerate(
            ((gate_hbm, w_gate), (up_hbm, w_up), (down_hbm, w_down))
        )
    ]
    own_load = pltpu.make_async_copy(weight_hbm, w_out.at[s], load_sem.at[3])
    own_load.start()
    for load in loads:
        load.start()
    greet(("sp", "tp"))

    partner = s + 1 - 2 * core
    ahead = s + 2 - 4 * core
    has_ahead = jnp.where(core == 0, z < chips - 1, z > 0)

    def along_line(b):
        return remote(w_out.at[b], w_out.at[b], w_line_send.at[b], w_recv.at[b], "sp", ahead)

    def to_partner(b):
        return remote(w_out.at[b], w_out.at[b], w_pair_send.at[b], w_recv.at[b], "sp", partner)

    def pass_on(b):
        @pl.when(has_ahead)
        def _():
            along_line(b).start()

    own_load.wait()
    to_partner(s).start()
    pass_on(s)

    def chip_behind(j):
        return z + (2 * core - 1) * j

    def serve(j, i):
        chip = chip_behind(j)

        @pl.when((chip >= 0) & (chip < chips))
        def _():
            b = chip * 2 + i
            along_line(b).wait_recv()
            to_partner(b).start()
            pass_on(b)

    head_count = cumul_ref.shape[1] // 2
    groups = (
        (query_a_ref, key_a_ref, cos_a_ref, sin_a_ref, rot_queries_a),
        (query_b_ref, key_b_ref, cos_b_ref, sin_b_ref, rot_queries_b),
    )
    size_a = query_a_ref.shape[1] // head_count
    dv = values_ref.shape[2] // head_count
    rows_i = lax.broadcasted_iota(jnp.int32, (count, count), 0)
    rows_j = lax.broadcasted_iota(jnp.int32, (count, count), 1)
    causal = rows_i >= rows_j

    def hop(c):
        return remote(
            departing.at[c], held.at[c], chain_send.at[c], chain_recv.at[c], "sp", (s + 1) % n_sp
        )

    pieces_of = []
    total_pieces = 0
    for g, (query_ref, key_ref, cos_ref, sin_ref, rot_ref) in enumerate(groups):
        size = query_ref.shape[1] // head_count
        for h in range(head_count):
            i = g * head_count + h
            lanes = slice(h * size, (h + 1) * size)
            cosine, sine = cos_ref[...], sin_ref[...]
            rot_q = turned(query_ref[:, lanes].astype(f32), cosine, sine).astype(bf16)
            rot_k = (turned(key_ref[:, lanes].astype(f32), cosine, sine) * size ** (-0.5)).astype(
                bf16
            )
            rot_ref[:, lanes] = rot_q
            column, row = cumul_ref[:, i : i + 1], cumul_rows_ref[i : i + 1, :]
            scores = lax.dot_general(
                rot_q, rot_k, (((1,), (1,)), ((), ())), preferred_element_type=f32
            )
            spread = column - row
            weight = jnp.where(causal, jnp.exp(jnp.where(causal, spread, 0.0)), 0.0)
            value = values_ref[g, :, h * dv : (h + 1) * dv]
            within[i] = jnp.dot(
                (scores * weight).astype(bf16), value, preferred_element_type=f32
            )
            last = cumul_ref[count - 1 : count, i : i + 1]
            carried = (rot_k.astype(f32) * jnp.exp(last - column)).astype(bf16)
            grown = lax.dot_general(
                carried, value, (((0,), (0,)), ((), ())), preferred_element_type=f32
            )
            mine = []
            for c in range(size // size_a):
                update[total_pieces] = grown[c * size_a : (c + 1) * size_a]
                fall[total_pieces] = jnp.broadcast_to(jnp.exp(last), (1, dv))
                mine.append(total_pieces)
                total_pieces += 1
            pieces_of.append(mine)

    to_line = partner
    to_partner(partner).wait_recv()
    pass_on(to_line)

    def step(c, _):
        @pl.when(s == 0)
        def _():
            held[c] = jnp.zeros(held.shape[1:], held.dtype)

        @pl.when(s > 0)
        def _():
            hop(c).wait_recv()

        @pl.when(s < n_sp - 1)
        def _():
            departing[c] = (fall[c] * held[c].astype(f32) + update[c]).astype(bf16)
            hop(c).start()

        return 0

    lax.fori_loop(0, total_pieces, step, 0)

    serve(1, 0)

    def heads_copy(g, k, source):
        block = heads.at[source, g]
        return remote(
            block, block, heads_send.at[g, k], heads_recv.at[g, source], "tp", (t + k) % n_tp
        )

    for g, (query_ref, _, _, _, rot_ref) in enumerate(groups):
        size = query_ref.shape[1] // head_count
        for h in range(head_count):
            i = g * head_count + h
            retained = within[i]
            cross = jnp.zeros((count, dv), f32)
            for c, piece in enumerate(pieces_of[i]):
                lanes = slice(h * size + c * size_a, h * size + (c + 1) * size_a)
                cross = cross + jnp.dot(rot_ref[:, lanes], held[piece], preferred_element_type=f32)
            retained = retained + cross * jnp.exp(cumul_ref[:, i : i + 1])
            scaled = retained * lax.rsqrt(
                jnp.mean(retained * retained, axis=1, keepdims=True) + EPS
            )
            lanes = slice(h * dv, (h + 1) * dv)
            gated = jax.nn.silu(gates_ref[g, :, lanes].astype(f32))
            heads[t, g, :, lanes] = (scaled * head_gain_ref[g : g + 1, lanes] * gated).astype(bf16)

        def heads_start(k, _, g=g):
            heads_copy(g, k, t).start()
            return 0

        lax.fori_loop(1, n_tp, heads_start, 0)

    serve(1, 1)
    for g in range(2):

        def heads_wait(k, _, g=g):
            heads_copy(g, k, (t + k) % n_tp).wait_recv()
            return 0

        lax.fori_loop(1, n_tp, heads_wait, 0)

    held_rows = w_out.shape[2]
    ratio = n_sp // n_tp

    def project_lanes(b, lanes):
        part = jnp.dot(heads[b // ratio, 0, :, lanes], w_out[b, 0], preferred_element_type=f32)
        part += jnp.dot(heads[b // ratio, 1, :, lanes], w_out[b, 1], preferred_element_type=f32)
        mix[...] += part

    def project(b):
        if held_rows % 128 == 0:
            project_lanes(
                b, pl.ds(pl.multiple_of((b % ratio) * held_rows, held_rows), held_rows)
            )
            return
        for r in range(ratio):

            @pl.when(b % ratio == r)
            def _(r=r):
                project_lanes(b, slice(r * held_rows, (r + 1) * held_rows))

    mix[...] = jnp.zeros_like(mix)
    for i in range(2):
        project(z * 2 + i)

    def project_chips(j, served):
        for i in range(2):
            if not served:
                serve(j, i)
        chip = chip_behind(j)

        @pl.when((chip >= 0) & (chip < chips))
        def _():
            for i in range(2):
                project(chip * 2 + i)

        other = z - (2 * core - 1) * j

        @pl.when((other >= 0) & (other < chips))
        def _():
            for i in range(2):
                to_partner(other * 2 + i).wait_recv()
                project(other * 2 + i)

    def project_far(j, _):
        project_chips(j, False)
        return 0

    def rows_of(p):
        return pl.ds(pl.multiple_of(p * cap, cap), cap)

    def group_rows(g, part=None):
        size = per_group * cap
        start = order[g] * size
        if part is None:
            return pl.ds(start, size)
        return pl.ds(start + part * (size // 2), size // 2)

    def square_copy(k, source):
        block, other = squares.at[source], (t + k) % n_tp
        return remote(block, block, sq_send.at[k], sq_recv.at[source], "tp", other)

    def dispatch(p, q):
        return remote(
            outgoing.at[rows_of(p)],
            arrived.at[t, rows_of(q)],
            disp_send.at[p],
            disp_recv.at[q],
            "sp",
            p,
        )

    def members(g, action):
        def body(j, _):
            action(order[g] * per_group + j)
            return 0

        lax.fori_loop(0, per_group, body, 0)

    def others(g, action):
        def guarded(p):
            @pl.when(p != s)
            def _():
                action(p)

        members(g, guarded)

    def finish_rows():
        stream = residual_ref[...].astype(f32) + mix[...].astype(bf16).astype(f32)
        stream_ref[...] = stream
        own = jnp.sum(stream * stream, axis=1, keepdims=True)
        squares[t] = jnp.broadcast_to(own, (count, count)).T[0:8, :]

        def square_start(k, _):
            square_copy(k, t).start()
            return 0

        def square_wait(k, _):
            square_copy(k, (t + k) % n_tp).wait()
            return 0

        lax.fori_loop(1, n_tp, square_start, 0)
        lax.fori_loop(1, n_tp, square_wait, 0)
        total = squares[0]
        for p in range(1, n_tp):
            total = total + squares[p]
        scale = lax.rsqrt(total[0:1, :] / (cols * n_tp) + EPS)
        scale = jnp.broadcast_to(scale, (count, count)).T[:, 0:1]
        normed = (stream_ref[...] * scale * gain_ref[...]).astype(bf16)
        slots = lax.broadcasted_iota(jnp.int32, (outgoing.shape[0], count), 0)
        select = (slots == target_ref[0:1, :]) | (slots == target_ref[1:2, :])
        select = jnp.where(select, 1.0, 0.0).astype(bf16)
        outgoing[...] = jnp.dot(select, normed, preferred_element_type=f32).astype(bf16)
        for g in range(GROUPS):
            others(g, lambda p: dispatch(p, s).start())
        arrived[t, rows_of(s)] = outgoing[rows_of(s)]

    lines = (
        [y * across + (x + k) % across for k in range(1, across)],
        [((y + k) % down) * across + x for k in range(1, down)],
    )
    direct = lines[0] + lines[1]

    def straight(buffer, sems, g, i, source, rows):
        block = buffer.at[source, rows]
        return remote(block, block, sems[0].at[g, i], sems[1].at[g, source], "tp", direct[i])

    def relayed(buffer, sems, g, part, i, source, target):
        block = buffer.at[source, group_rows(g, part)]
        return remote(
            block, block, sems[2].at[g, part, i], sems[3].at[g, source, part], "tp", target
        )

    def relay(buffer, sems, g):
        for part in range(2):
            for k, source in enumerate(lines[part]):
                i = k if part == 0 else len(lines[0]) + k
                straight(buffer, sems, g, i, source, group_rows(g)).wait_recv()
                for j, target in enumerate(lines[1 - part]):
                    relayed(
                        buffer, sems, g, part, k * len(lines[1 - part]) + j, source, target
                    ).start()

    def place_of(k):
        return ((y + k // across) % down) * across + (x + k % across) % across

    def wait_relayed(buffer, sems, g, k):
        @pl.when((k // across) * (k % across) > 0)
        def _():
            source = place_of(k)
            for part in range(2):
                relayed(buffer, sems, g, part, 0, source, source).wait_recv()

    def finish_sends(buffer, sems, g):
        for i in range(len(direct)):
            straight(buffer, sems, g, i, t, group_rows(g)).wait_send()
        for part in range(2):
            for i in range(len(lines[0]) * len(lines[1])):
                relayed(buffer, sems, g, part, i, t, direct[0]).wait_send()

    arrived_sems = (fwd_send, fwd_recv, fwd_relay_send, fwd_relay_recv)
    hidden_sems = (hid_send, hid_recv, hid_relay_send, hid_relay_recv)

    def forward(g):
        def block(p):
            @pl.when(p != s)
            def _():
                dispatch(p, p).wait_recv()

            for i in range(len(direct)):
                straight(arrived, arrived_sems, g, i, t, rows_of(p)).start()

        members(g, block)

    def through_units(g):
        acc_a[...] = jnp.zeros_like(acc_a)
        acc_b[...] = jnp.zeros_like(acc_b)

        def body(k, _):
            wait_relayed(arrived, arrived_sems, g, k)
            p = place_of(k)
            part = pl.ds(pl.multiple_of(p * cols, cols), cols)
            rows = arrived[p, group_rows(g)]
            acc_a[...] += jnp.dot(rows, w_gate[part, :], preferred_element_type=f32)
            acc_b[...] += jnp.dot(rows, w_up[part, :], preferred_element_type=f32)
            return 0

        lax.fori_loop(0, n_tp, body, 0)
        hidden[t, group_rows(g)] = (jax.nn.silu(acc_a[...]) * acc_b[...]).astype(bf16)
        for i in range(len(direct)):
            straight(hidden, hidden_sems, g, i, t, group_rows(g)).start()

    def give_back(p, q):
        return remote(
            result.at[rows_of(p)], returned.at[rows_of(q)], ret_send.at[p], ret_recv.at[q], "sp", p
        )

    def through_down(g):
        acc_c[...] = jnp.zeros_like(acc_c)

        def body(k, _):
            wait_relayed(hidden, hidden_sems, g, k)
            p = place_of(k)
            part = pl.ds(pl.multiple_of(p * units, units), units)
            acc_c[...] += jnp.dot(
                hidden[p, group_rows(g)], w_down[part, :], preferred_element_type=f32
            )
            return 0

        lax.fori_loop(0, n_tp, body, 0)
        result[group_rows(g)] = acc_c[...].astype(bf16)
        others(g, lambda p: give_back(p, s).start())

    relay_rows = lambda g: relay(arrived, arrived_sems, g)
    relay_hidden = lambda g: relay(hidden, hidden_sems, g)

    inner_lo, inner_hi = chips // 4, chips - chips // 4
    inner = (z >= inner_lo) & (z < inner_hi)
    if chips > 1:
        project_chips(1, True)
    lax.fori_loop(2, inner_hi, project_far, 0)

    @pl.when(inner)
    def _():
        finish_rows()

    half = GROUPS // 2
    for g in range(half):
        forward(g)
    for g in range(half):
        relay_rows(g)
    for load in loads:
        load.wait()
    for g in range(half):
        through_units(g)

    lax.fori_loop(inner_hi, chips, project_far, 0)

    @pl.when(jnp.logical_not(inner))
    def _():
        finish_rows()

    for g in range(half):
        relay_hidden(g)
    for g in range(half):
        through_down(g)
    for g in range(half, GROUPS):
        forward(g)
    for g in range(half, GROUPS):
        relay_rows(g)
    for g in range(half, GROUPS):
        through_units(g)
    for g in range(half, GROUPS):
        relay_hidden(g)
    for g in range(half, GROUPS):
        through_down(g)

    returned[rows_of(s)] = result[rows_of(s)]
    for g in range(GROUPS):
        others(g, lambda p: give_back(p, p).wait_recv())
    out_ref[...] = returned[...]

    @pl.when(s < n_sp - 1)
    def _():
        def gone(c, _):
            hop(c).wait_send()
            return 0

        lax.fori_loop(0, total_pieces, gone, 0)

    for g in range(2):

        def heads_gone(k, _, g=g):
            heads_copy(g, k, t).wait_send()
            return 0

        lax.fori_loop(1, n_tp, heads_gone, 0)

    def passed(j, _):
        chip = chip_behind(j)

        @pl.when((chip >= 0) & (chip < chips))
        def _():
            for i in range(2):
                b = chip * 2 + i

                @pl.when(has_ahead)
                def _():
                    along_line(b).wait_send()

                @pl.when((b == s) | (j > 0))
                def _():
                    to_partner(b).wait_send()

        return 0

    lax.fori_loop(0, chips, passed, 0)
    for g in range(GROUPS):
        others(g, lambda p: dispatch(p, s).wait_send())
        others(g, lambda p: give_back(p, s).wait_send())
        finish_sends(arrived, arrived_sems, g)
        finish_sends(hidden, hidden_sems, g)


def tables(positions, size):
    half = size // 2
    inverse = jnp.power(THETA, -jnp.arange(half, dtype=jnp.float32) * 2.0 / size)
    inverse = jnp.concatenate([inverse, inverse])
    sign = jnp.where(jnp.arange(size) < half, -1.0, 1.0)
    angles = positions[:, None] * inverse[None, :]
    return jnp.cos(angles), jnp.sin(angles) * sign[None, :]


def per_device(
    residual,
    query_small,
    key_narrow_group,
    query_large,
    key_large,
    values,
    gates,
    log_decay,
    head_gain,
    out_weight,
    norm_gain,
    routes,
    route_weight,
    expert_gate,
    expert_up,
    expert_down,
):
    n_sp, n_tp = lax.axis_size("sp"), lax.axis_size("tp")
    row_count, cols = residual.shape
    head_count = log_decay.shape[2]
    bf16, f32 = jnp.bfloat16, jnp.float32
    positions = (lax.axis_index("sp") * row_count + jnp.arange(row_count, dtype=jnp.int32)).astype(
        f32
    )
    size_a, size_b = query_small.shape[1] // head_count, query_large.shape[1] // head_count
    cos_a, sin_a = tables(positions, size_a)
    cos_b, sin_b = tables(positions, size_b)
    cumul = jnp.cumsum(log_decay.reshape(row_count, 2 * head_count), axis=0)

    experts = n_sp
    capacity = 4 * row_count // experts
    slots = experts * capacity
    numbers = jnp.arange(experts, dtype=jnp.int32)
    named = [(routes[:, c][:, None] == numbers[None, :]) for c in range(2)]
    counted = (named[0].astype(bf16) + named[1].astype(bf16))
    earlier = jnp.arange(row_count)[:, None] > jnp.arange(row_count)[None, :]
    before = jnp.dot(earlier.astype(bf16), counted, preferred_element_type=f32)
    target = [
        routes[:, c] * capacity
        + jnp.sum(jnp.where(named[c], before, 0.0), axis=1).astype(jnp.int32)
        for c in range(2)
    ]

    pieces = head_count * (1 + size_b // size_a)
    value_size = values.shape[2] // head_count
    width, units = expert_gate.shape[1:]
    dma = pltpu.SemaphoreType.DMA
    across, down = grid_of(n_tp)
    straights, relays = across + down - 2, (across - 1) * (down - 1)
    vmem = pl.BlockSpec(memory_space=pltpu.VMEM)
    hbm = pl.BlockSpec(memory_space=pl.ANY)
    returned, stream = pl.pallas_call(
        layer_kernel,
        out_shape=(
            jax.ShapeDtypeStruct((slots, cols), bf16),
            jax.ShapeDtypeStruct((row_count, cols), f32),
        ),
        in_specs=[vmem] * 16 + [hbm] * 4,
        out_specs=(vmem, vmem),
        scratch_shapes=[
            pltpu.VMEM(query_small.shape, bf16),
            pltpu.VMEM(query_large.shape, bf16),
            pltpu.VMEM((2 * head_count, row_count, value_size), f32),
            pltpu.VMEM((pieces, size_a, value_size), f32),
            pltpu.VMEM((pieces, 1, value_size), f32),
            pltpu.VMEM((pieces, size_a, value_size), bf16),
            pltpu.VMEM((pieces, size_a, value_size), bf16),
            pltpu.VMEM((n_tp, 2, row_count, values.shape[2]), bf16),
            pltpu.VMEM((n_sp,) + out_weight.shape, bf16),
            pltpu.VMEM((row_count, cols), f32),
            pltpu.VMEM((width, units), bf16),
            pltpu.VMEM((width, units), bf16),
            pltpu.VMEM(expert_down.shape[1:], bf16),
            pltpu.VMEM((n_tp, 8, row_count), f32),
            pltpu.VMEM((slots, cols), bf16),
            pltpu.VMEM((n_tp, slots, cols), bf16),
            pltpu.VMEM((n_tp, slots, units), bf16),
            pltpu.VMEM((slots, cols), bf16),
            pltpu.VMEM((slots, cols), bf16),
            pltpu.VMEM((slots // GROUPS, units), f32),
            pltpu.VMEM((slots // GROUPS, units), f32),
            pltpu.VMEM((slots // GROUPS, cols), f32),
            dma((4,)),
            dma((pieces,)),
            dma((pieces,)),
            dma((2, n_tp)),
            dma((2, n_tp)),
            dma((n_sp,)),
            dma((n_sp,)),
            dma((n_sp,)),
            dma((n_tp,)),
            dma((n_tp,)),
            dma((n_sp,)),
            dma((n_sp,)),
            dma((GROUPS, straights)),
            dma((GROUPS, n_tp)),
            dma((GROUPS, 2, relays)),
            dma((GROUPS, n_tp, 2)),
            dma((GROUPS, straights)),
            dma((GROUPS, n_tp)),
            dma((GROUPS, 2, relays)),
            dma((GROUPS, n_tp, 2)),
            dma((n_sp,)),
            dma((n_sp,)),
        ],
        compiler_params=pltpu.CompilerParams(
            collective_id=0, has_side_effects=True, vmem_limit_bytes=58 * 2**20
        ),
    )(
        residual,
        query_small,
        key_narrow_group,
        query_large,
        key_large,
        jnp.swapaxes(values, 0, 1),
        jnp.swapaxes(gates, 0, 1),
        cos_a,
        sin_a,
        cos_b,
        sin_b,
        cumul,
        cumul.T,
        head_gain,
        norm_gain[None, :],
        jnp.stack(target),
        out_weight,
        expert_gate,
        expert_up,
        expert_down,
    )
    ids = jnp.arange(slots, dtype=jnp.int32)[None, :]
    picks = [
        jnp.dot(
            (target[c][:, None] == ids).astype(bf16), returned, preferred_element_type=f32
        )
        for c in range(2)
    ]
    routed = route_weight[:, 0:1] * picks[0] + route_weight[:, 1:2] * picks[1]
    return (stream + routed).astype(bf16)


def solution(mesh):
    placed = (
        P("sp", "tp"),
        P("sp", "tp"),
        P("sp", "tp"),
        P("sp", "tp"),
        P("sp", "tp"),
        P("sp", None, "tp"),
        P("sp", None, "tp"),
        P("sp", None, "tp"),
        P(None, "tp"),
        P(None, "sp", "tp"),
        P("tp"),
        P("sp", None),
        P("sp", None),
        P("sp", None, "tp"),
        P("sp", None, "tp"),
        P("sp", None, "tp"),
    )
    return jax.shard_map(
        per_device, mesh=mesh, in_specs=placed, out_specs=P("sp", "tp"), check_vma=False
    )
```

```python
import jax
import jax.numpy as jnp
import numpy as np
from jax import lax
from jax.experimental import pallas as pl
from jax.experimental.pallas import tpu as pltpu
from jax.sharding import PartitionSpec as P

MESH = pl.DeviceIdType.MESH


EPS = 1e-06
THETA = 10000.0


def greet(axes):
    barrier = pltpu.get_barrier_semaphore()
    total = 0
    for axis in axes:
        count, me = lax.axis_size(axis), lax.axis_index(axis)

        def signal(k, _, axis=axis, count=count, me=me):
            pl.semaphore_signal(
                barrier, inc=1, device_id={axis: (me + k) % count}, device_id_type=MESH
            )
            return 0

        lax.fori_loop(1, count, signal, 0)
        total += count - 1
    pl.semaphore_wait(barrier, total)


def remote(source, target, send_sem, recv_sem, axis, index):
    return pltpu.make_async_remote_copy(
        src_ref=source,
        dst_ref=target,
        send_sem=send_sem,
        recv_sem=recv_sem,
        device_id={axis: index},
        device_id_type=MESH,
    )


GROUPS = 8


def grid_of(count):
    across = max(k for k in range(1, count + 1) if count % k == 0 and k * k <= count)
    return across, count // across


QUARTERS = ((0, 2, 3, 1), (1, 2, 0, 3), (2, 1, 3, 0), (3, 1, 0, 2))
SENDS = ((1, 3, 2), (2, 3, 0), (1, 0, 3), (2, 0, 1))
ORDER = tuple(
    (k,) + tuple(2 * q + i for q in QUARTERS[k // 2][1:] for i in range(2)) + (k ^ 1,)
    for k in range(GROUPS)
)


def turned(block, cosine, sine):
    half = block.shape[1] // 2
    if half % 128:
        swapped = pltpu.roll(block, half, axis=1)
    else:
        swapped = jnp.concatenate([block[:, half:], block[:, :half]], axis=1)
    return block * cosine + swapped * sine


def layer_kernel(
    residual_ref,
    query_a_ref,
    key_a_ref,
    query_b_ref,
    key_b_ref,
    values_ref,
    gates_ref,
    turn_a_ref,
    start_a_ref,
    turn_b_ref,
    start_b_ref,
    decay_ref,
    head_gain_ref,
    gain_ref,
    routes_ref,
    route_weight_ref,
    weight_hbm,
    gate_hbm,
    up_hbm,
    down_hbm,
    out_ref,
    stream_ref,
    cumul_ref,
    cumul_rows_ref,
    rot_queries_a,
    rot_queries_b,
    within,
    update,
    fall,
    held,
    departing,
    heads,
    w_out,
    mix,
    w_gate,
    w_up,
    w_down,
    squares,
    outgoing,
    arrived,
    hidden,
    far_heads,
    far_out,
    far_in,
    result,
    returned,
    acc_a,
    acc_b,
    acc_c,
    load_sem,
    chain_send,
    chain_recv,
    heads_send,
    heads_recv,
    w_line_send,
    w_pair_send,
    w_recv,
    far_send,
    far_recv,
    sq_send,
    sq_recv,
    disp_send,
    disp_recv,
    fwd_send,
    fwd_recv,
    fwd_relay_send,
    fwd_relay_recv,
    hid_send,
    hid_recv,
    hid_relay_send,
    hid_relay_recv,
    ret_send,
    ret_recv,
):
    n_sp, n_tp = lax.axis_size("sp"), lax.axis_size("tp")
    s, t = lax.axis_index("sp"), lax.axis_index("tp")
    bf16, f32 = jnp.bfloat16, jnp.float32
    per_group = n_sp // GROUPS
    across, down = grid_of(n_tp)
    x, y = t % across, t // across
    cap = outgoing.shape[0] // n_sp
    cols = stream_ref.shape[1]
    units = w_gate.shape[1]
    count = stream_ref.shape[0]
    chips = n_sp // 2
    z, core = s // 2, s % 2
    loads = [
        pltpu.make_async_copy(source.at[0], target, load_sem.at[i])
        for i, (source, target) in enumerate(
            ((gate_hbm, w_gate), (up_hbm, w_up), (down_hbm, w_down))
        )
    ]
    own_load = pltpu.make_async_copy(weight_hbm, w_out.at[s], load_sem.at[3])
    own_load.start()
    for load in loads:
        load.start()
    with jax.named_scope("greet"):
        greet(("sp", "tp"))

    partner = s + 1 - 2 * core
    ahead = s + 2 - 4 * core
    has_ahead = jnp.where(core == 0, z < chips - 1, z > 0)

    def along_line(b):
        return remote(w_out.at[b], w_out.at[b], w_line_send.at[b], w_recv.at[b], "sp", ahead)

    def to_partner(b):
        return remote(w_out.at[b], w_out.at[b], w_pair_send.at[b], w_recv.at[b], "sp", partner)

    reach = chips - 2

    def pass_on(b, j):
        @pl.when(has_ahead & (j < reach))
        def _():
            along_line(b).start()

    with jax.named_scope("own"):
        own_load.wait()
    to_partner(s).start()
    pass_on(s, 0)

    def chip_behind(j):
        return z + (2 * core - 1) * j

    def serve(j, i):
        chip = chip_behind(j)

        @pl.when((chip >= 0) & (chip < chips))
        def _():
            b = chip * 2 + i
            along_line(b).wait_recv()
            to_partner(b).start()
            pass_on(b, j)

    head_count = decay_ref.shape[0] // 2
    groups = (
        (query_a_ref, key_a_ref, turn_a_ref, start_a_ref, rot_queries_a),
        (query_b_ref, key_b_ref, turn_b_ref, start_b_ref, rot_queries_b),
    )
    size_a = query_a_ref.shape[1] // head_count
    dv = values_ref.shape[2] // head_count
    rows_i = lax.broadcasted_iota(jnp.int32, (count, count), 0)
    rows_j = lax.broadcasted_iota(jnp.int32, (count, count), 1)
    causal = rows_i >= rows_j
    exact = lax.Precision.HIGHEST
    cumul_rows_ref[...] = jnp.dot(
        decay_ref[...],
        jnp.where(rows_i <= rows_j, 1.0, 0.0),
        precision=exact,
        preferred_element_type=f32,
    )
    cumul_ref[...] = lax.dot_general(
        jnp.where(causal, 1.0, 0.0),
        decay_ref[...],
        (((1,), (1,)), ((), ())),
        precision=exact,
        preferred_element_type=f32,
    )

    def hop(c):
        return remote(
            departing.at[c], held.at[c], chain_send.at[c], chain_recv.at[c], "sp", (s + 1) % n_sp
        )

    pieces_of = []
    total_pieces = 0
    for g, (query_ref, key_ref, turn_ref, start_ref, rot_ref) in enumerate(groups):
        size = query_ref.shape[1] // head_count
        cos_start, sin_start = start_ref[0, pl.ds(s, 1), :], start_ref[1, pl.ds(s, 1), :]
        cosine = cos_start * turn_ref[0] - sin_start * turn_ref[1]
        sine = sin_start * turn_ref[0] + cos_start * turn_ref[1]
        for h in range(head_count):
            i = g * head_count + h
            lanes = slice(h * size, (h + 1) * size)
            rot_q = turned(query_ref[:, lanes].astype(f32), cosine, sine).astype(bf16)
            rot_k = (turned(key_ref[:, lanes].astype(f32), cosine, sine) * size ** (-0.5)).astype(
                bf16
            )
            rot_ref[:, lanes] = rot_q
            column, row = cumul_ref[:, i : i + 1], cumul_rows_ref[i : i + 1, :]
            scores = lax.dot_general(
                rot_q, rot_k, (((1,), (1,)), ((), ())), preferred_element_type=f32
            )
            spread = column - row
            weight = jnp.where(causal, jnp.exp(jnp.where(causal, spread, 0.0)), 0.0)
            value = values_ref[:, g, h * dv : (h + 1) * dv]
            within[i] = jnp.dot(
                (scores * weight).astype(bf16), value, preferred_element_type=f32
            )
            last = cumul_ref[count - 1 : count, i : i + 1]
            carried = (rot_k.astype(f32) * jnp.exp(last - column)).astype(bf16)
            grown = lax.dot_general(
                carried, value, (((0,), (0,)), ((), ())), preferred_element_type=f32
            )
            mine = []
            for c in range(size // size_a):
                update[total_pieces] = grown[c * size_a : (c + 1) * size_a]
                fall[total_pieces] = jnp.broadcast_to(jnp.exp(last), (1, dv))
                mine.append(total_pieces)
                total_pieces += 1
            pieces_of.append(mine)

    to_line = partner
    with jax.named_scope("pair"):
        to_partner(partner).wait_recv()
    pass_on(to_line, 0)

    def step(c, _):
        @pl.when(s == 0)
        def _():
            held[c] = jnp.zeros(held.shape[1:], held.dtype)

        @pl.when(s > 0)
        def _():
            hop(c).wait_recv()

        @pl.when(s < n_sp - 1)
        def _():
            departing[c] = (fall[c] * held[c].astype(f32) + update[c]).astype(bf16)
            hop(c).start()

        return 0

    with jax.named_scope("chain"):
        lax.fori_loop(0, total_pieces, step, 0)

    with jax.named_scope("serve0"):
        serve(1, 0)

    def heads_copy(g, k, source):
        block = heads.at[source, g]
        return remote(
            block, block, heads_send.at[g, k], heads_recv.at[g, source], "tp", (t + k) % n_tp
        )

    for g, (query_ref, _, _, _, rot_ref) in enumerate(groups):
        size = query_ref.shape[1] // head_count
        for h in range(head_count):
            i = g * head_count + h
            retained = within[i]
            cross = jnp.zeros((count, dv), f32)
            for c, piece in enumerate(pieces_of[i]):
                lanes = slice(h * size + c * size_a, h * size + (c + 1) * size_a)
                cross = cross + jnp.dot(rot_ref[:, lanes], held[piece], preferred_element_type=f32)
            retained = retained + cross * jnp.exp(cumul_ref[:, i : i + 1])
            scaled = retained * lax.rsqrt(
                jnp.mean(retained * retained, axis=1, keepdims=True) + EPS
            )
            lanes = slice(h * dv, (h + 1) * dv)
            gated = jax.nn.silu(gates_ref[:, g, lanes].astype(f32))
            heads[t, g, :, lanes] = (scaled * head_gain_ref[g : g + 1, lanes] * gated).astype(bf16)

        def heads_start(k, _, g=g):
            heads_copy(g, k, t).start()
            return 0

        lax.fori_loop(1, n_tp, heads_start, 0)

    with jax.named_scope("serve1"):
        serve(1, 1)
    for g in range(2):

        def heads_wait(k, _, g=g):
            heads_copy(g, k, (t + k) % n_tp).wait_recv()
            return 0

        with jax.named_scope("headswait"):
            lax.fori_loop(1, n_tp, heads_wait, 0)

    at_low, at_high = z == 0, z == chips - 1
    near_low, near_high = z == 1, z == chips - 2

    def far_pair(low, shift, action):
        @pl.when(low)
        def _():
            action(shift)

    def ask(shift):
        return remote(
            heads.at[chips - 1 - z], far_heads, far_send.at[0], far_recv.at[0], "sp", s + shift
        )

    def answer(shift):
        return remote(far_out, far_in, far_send.at[1], far_recv.at[1], "sp", s + shift)

    far_pair(at_low, 2, lambda shift: ask(shift).start())
    far_pair(at_high, -2, lambda shift: ask(shift).start())

    held_rows = w_out.shape[2]
    ratio = n_sp // n_tp

    def project_lanes(b, lanes):
        part = jnp.dot(heads[b // ratio, 0, :, lanes], w_out[b, 0], preferred_element_type=f32)
        part += jnp.dot(heads[b // ratio, 1, :, lanes], w_out[b, 1], preferred_element_type=f32)
        mix[...] += part

    def project(b):
        if held_rows % 128 == 0:
            project_lanes(
                b, pl.ds(pl.multiple_of((b % ratio) * held_rows, held_rows), held_rows)
            )
            return
        for r in range(ratio):

            @pl.when(b % ratio == r)
            def _(r=r):
                project_lanes(b, slice(r * held_rows, (r + 1) * held_rows))

    mix[...] = jnp.zeros_like(mix)
    for i in range(2):
        project(z * 2 + i)

    def project_chips(j, served):
        for i in range(2):
            if not served:
                serve(j, i)
        chip = chip_behind(j)

        @pl.when((chip >= 0) & (chip < chips))
        def _():
            for i in range(2):
                project(chip * 2 + i)

        other = z - (2 * core - 1) * j

        @pl.when((other >= 0) & (other < chips))
        def _():
            for i in range(2):
                to_partner(other * 2 + i).wait_recv()
                project(other * 2 + i)

    def project_far(j, _):
        project_chips(j, False)
        return 0

    def project_edge(shift):
        ask(shift).wait_recv()
        far = chips - 1 if shift < 0 else 0
        part = jnp.zeros((count, cols), f32)
        for i in range(2):
            lanes = slice(i * held_rows, (i + 1) * held_rows)
            for g in range(2):
                part += jnp.dot(
                    far_heads[g, :, lanes], w_out[2 * far + i, g], preferred_element_type=f32
                )
        far_out[...] = part.astype(bf16)
        answer(shift).start()

    def add_edge(shift):
        answer(shift).wait_recv()
        mix[...] += far_in[...].astype(f32)

    def rows_of(p):
        return pl.ds(pl.multiple_of(p * cap, cap), cap)

    eighth, quarter = s // per_group, s // (n_sp // 4)

    def group_base(g):
        base = ORDER[0][g]
        for k in range(1, GROUPS):
            base = jnp.where(eighth == k, ORDER[k][g], base)
        return base * per_group

    def group_rows(g, part=None):
        size = per_group * cap
        start = pl.multiple_of(group_base(g) * cap, size)
        if part is None:
            return pl.ds(start, size)
        return pl.ds(pl.multiple_of(start + part * (size // 2), size // 2), size // 2)

    def square_copy(k, source):
        block, other = squares.at[source], (t + k) % n_tp
        return remote(block, block, sq_send.at[k], sq_recv.at[source], "tp", other)

    def dispatch(p, q):
        return remote(
            outgoing.at[rows_of(p)],
            arrived.at[t, rows_of(q)],
            disp_send.at[p],
            disp_recv.at[q],
            "sp",
            p,
        )

    def members(g, action):
        def body(j, _):
            action(group_base(g) + j)
            return 0

        lax.fori_loop(0, per_group, body, 0)

    def others(g, action):
        def guarded(p):
            @pl.when(p != s)
            def _():
                action(p)

        members(g, guarded)

    def choice(c):
        numbers = lax.broadcasted_iota(jnp.int32, (n_sp, count), 0)
        named = [numbers == routes_ref[k : k + 1, :] for k in range(2)]
        counted = [jnp.where(mask, 1.0, 0.0).astype(bf16) for mask in named]
        earlier = jnp.where(rows_i < rows_j, 1.0, 0.0).astype(bf16)
        before = jnp.dot(counted[0] + counted[1], earlier, preferred_element_type=f32)
        slot = jnp.sum(jnp.where(named[c], before, 0.0), axis=0, keepdims=True)
        target = routes_ref[c : c + 1, :] * cap + slot.astype(jnp.int32)
        slots = lax.broadcasted_iota(jnp.int32, (outgoing.shape[0], count), 0)
        return jnp.where(slots == target, 1.0, 0.0).astype(bf16)

    def finish_rows():
        stream = residual_ref[...].astype(f32) + mix[...].astype(bf16).astype(f32)
        stream_ref[...] = stream
        own = jnp.sum(stream * stream, axis=1, keepdims=True)
        squares[t] = jnp.broadcast_to(own, (count, count)).T[0:8, :]

        def square_start(k, _):
            square_copy(k, t).start()
            return 0

        def square_wait(k, _):
            square_copy(k, (t + k) % n_tp).wait()
            return 0

        lax.fori_loop(1, n_tp, square_start, 0)
        lax.fori_loop(1, n_tp, square_wait, 0)
        total = squares[0]
        for p in range(1, n_tp):
            total = total + squares[p]
        scale = lax.rsqrt(total[0:1, :] / (cols * n_tp) + EPS)
        scale = jnp.broadcast_to(scale, (count, count)).T[:, 0:1]
        normed = (stream_ref[...] * scale * gain_ref[...]).astype(bf16)
        select = choice(0) + choice(1)
        outgoing[...] = jnp.dot(select, normed, preferred_element_type=f32).astype(bf16)
        arrived[t, rows_of(s)] = outgoing[rows_of(s)]

    def dispatch_to(q):
        def body(j, _):
            p = q * (n_sp // 4) + j

            @pl.when(p != s)
            def _():
                dispatch(p, s).start()

            return 0

        lax.fori_loop(0, n_sp // 4, body, 0)

    def dispatch_stage(i):
        for q in range(4):

            @pl.when(quarter == q)
            def _(q=q):
                dispatch_to(SENDS[q][i])

    lines = (
        [y * across + (x + k) % across for k in range(1, across)],
        [((y + k) % down) * across + x for k in range(1, down)],
    )
    direct = lines[0] + lines[1]

    def straight(buffer, sems, g, i, source, rows):
        block = buffer.at[source, rows]
        return remote(block, block, sems[0].at[g, i], sems[1].at[g, source], "tp", direct[i])

    def relayed(buffer, sems, g, part, i, source, target):
        block = buffer.at[source, group_rows(g, part)]
        return remote(
            block, block, sems[2].at[g, part, i], sems[3].at[g, source, part], "tp", target
        )

    def relay(buffer, sems, g):
        for part in range(2):
            for k, source in enumerate(lines[part]):
                i = k if part == 0 else len(lines[0]) + k
                straight(buffer, sems, g, i, source, group_rows(g)).wait_recv()
                for j, target in enumerate(lines[1 - part]):
                    relayed(
                        buffer, sems, g, part, k * len(lines[1 - part]) + j, source, target
                    ).start()

    def place_of(k):
        return ((y + k // across) % down) * across + (x + k % across) % across

    def wait_relayed(buffer, sems, g, k):
        @pl.when((k // across) * (k % across) > 0)
        def _():
            source = place_of(k)
            for part in range(2):
                relayed(buffer, sems, g, part, 0, source, source).wait_recv()

    def finish_sends(buffer, sems, g):
        for i in range(len(direct)):
            straight(buffer, sems, g, i, t, group_rows(g)).wait_send()
        for part in range(2):
            for i in range(len(lines[0]) * len(lines[1])):
                relayed(buffer, sems, g, part, i, t, direct[0]).wait_send()

    arrived_sems = (fwd_send, fwd_recv, fwd_relay_send, fwd_relay_recv)
    hidden_sems = (hid_send, hid_recv, hid_relay_send, hid_relay_recv)

    def forward(g):
        def block(p):
            @pl.when(p != s)
            def _():
                dispatch(p, p).wait_recv()

            for i in range(len(direct)):
                straight(arrived, arrived_sems, g, i, t, rows_of(p)).start()

        with jax.named_scope("forward"):
            members(g, block)

    def through_units(g):
        acc_a[...] = jnp.zeros_like(acc_a)
        acc_b[...] = jnp.zeros_like(acc_b)

        def body(k, _):
            wait_relayed(arrived, arrived_sems, g, k)
            p = place_of(k)
            part = pl.ds(pl.multiple_of(p * cols, cols), cols)
            rows = arrived[p, group_rows(g)]
            acc_a[...] += jnp.dot(rows, w_gate[part, :], preferred_element_type=f32)
            acc_b[...] += jnp.dot(rows, w_up[part, :], preferred_element_type=f32)
            return 0

        with jax.named_scope("units"):
            lax.fori_loop(0, n_tp, body, 0)
        hidden[t, group_rows(g)] = (jax.nn.silu(acc_a[...]) * acc_b[...]).astype(bf16)
        for i in range(len(direct)):
            straight(hidden, hidden_sems, g, i, t, group_rows(g)).start()

    def give_back(p, q):
        return remote(
            result.at[rows_of(p)], returned.at[rows_of(q)], ret_send.at[p], ret_recv.at[q], "sp", p
        )

    def through_down(g):
        acc_c[...] = jnp.zeros_like(acc_c)

        def body(k, _):
            wait_relayed(hidden, hidden_sems, g, k)
            p = place_of(k)
            part = pl.ds(pl.multiple_of(p * units, units), units)
            acc_c[...] += jnp.dot(
                hidden[p, group_rows(g)], w_down[part, :], preferred_element_type=f32
            )
            return 0

        with jax.named_scope("down"):
            lax.fori_loop(0, n_tp, body, 0)
        result[group_rows(g)] = acc_c[...].astype(bf16)
        others(g, lambda p: give_back(p, s).start())

    def relay_rows(g):
        with jax.named_scope("relay_rows"):
            relay(arrived, arrived_sems, g)

    def relay_hidden(g):
        with jax.named_scope("relay_hidden"):
            relay(hidden, hidden_sems, g)

    with jax.named_scope("proj1"):
        project_chips(1, True)
    with jax.named_scope("proj2"):
        lax.fori_loop(2, reach + 1, project_far, 0)
    far_pair(near_low, -2, project_edge)
    far_pair(near_high, 2, project_edge)
    with jax.named_scope("edge"):
        far_pair(at_low, 2, add_edge)
        far_pair(at_high, -2, add_edge)
    with jax.named_scope("finish"):
        finish_rows()
    dispatch_stage(0)
    dispatch_to(quarter)
    for load in loads:
        load.wait()
    for step in range(GROUPS + 4):
        for late, action in enumerate(
            (forward, relay_rows, through_units, relay_hidden, through_down)
        ):
            if 0 <= step - late < GROUPS:
                action(step - late)
            if late == 1 and step in (1, 3):
                dispatch_stage((step + 1) // 2)

    returned[rows_of(s)] = result[rows_of(s)]
    with jax.named_scope("back"):
        for g in range(GROUPS):
            others(g, lambda p: give_back(p, p).wait_recv())
    total = stream_ref[...]
    for c in range(2):
        pick = lax.dot_general(
            choice(c), returned[...], (((0,), (0,)), ((), ())), preferred_element_type=f32
        )
        share = jnp.broadcast_to(route_weight_ref[c : c + 1, :], (count, count)).T[:, 0:1]
        total = total + share * pick
    out_ref[...] = total.astype(bf16)

    @pl.when(s < n_sp - 1)
    def _():
        def gone(c, _):
            hop(c).wait_send()
            return 0

        lax.fori_loop(0, total_pieces, gone, 0)

    for g in range(2):

        def heads_gone(k, _, g=g):
            heads_copy(g, k, t).wait_send()
            return 0

        lax.fori_loop(1, n_tp, heads_gone, 0)

    def passed(j, _):
        chip = chip_behind(j)

        @pl.when((chip >= 0) & (chip < chips))
        def _():
            for i in range(2):
                b = chip * 2 + i

                @pl.when(has_ahead & (j < reach))
                def _():
                    along_line(b).wait_send()

                @pl.when((b == s) | (j > 0))
                def _():
                    to_partner(b).wait_send()

        return 0

    lax.fori_loop(0, reach + 1, passed, 0)
    far_pair(at_low, 2, lambda shift: ask(shift).wait_send())
    far_pair(at_high, -2, lambda shift: ask(shift).wait_send())
    far_pair(near_low, -2, lambda shift: answer(shift).wait_send())
    far_pair(near_high, 2, lambda shift: answer(shift).wait_send())
    for g in range(GROUPS):
        others(g, lambda p: dispatch(p, s).wait_send())
        others(g, lambda p: give_back(p, s).wait_send())
        finish_sends(arrived, arrived_sems, g)
        finish_sends(hidden, hidden_sems, g)


def tables(rows, blocks, size):
    half = size // 2
    inverse = np.power(THETA, -np.arange(half) * 2.0 / size)
    inverse = np.concatenate([inverse, inverse])
    sign = np.where(np.arange(size) < half, -1.0, 1.0)

    def at(positions):
        angles = positions[:, None] * inverse[None, :]
        return jnp.asarray(np.stack([np.cos(angles), np.sin(angles) * sign]), jnp.float32)

    return at(np.arange(rows)), at(np.arange(blocks) * rows)


def per_device(
    residual,
    query_small,
    key_narrow_group,
    query_large,
    key_large,
    values,
    gates,
    log_decay,
    head_gain,
    out_weight,
    norm_gain,
    routes,
    route_weight,
    expert_gate,
    expert_up,
    expert_down,
):
    n_sp, n_tp = lax.axis_size("sp"), lax.axis_size("tp")
    row_count, cols = residual.shape
    head_count = log_decay.shape[2]
    bf16, f32 = jnp.bfloat16, jnp.float32
    size_a, size_b = query_small.shape[1] // head_count, query_large.shape[1] // head_count
    turn_a, start_a = tables(row_count, n_sp, size_a)
    turn_b, start_b = tables(row_count, n_sp, size_b)
    slots = 4 * row_count
    pieces = head_count * (1 + size_b // size_a)
    value_size = values.shape[2] // head_count
    width, units = expert_gate.shape[1:]
    dma = pltpu.SemaphoreType.DMA
    across, down = grid_of(n_tp)
    straights, relays = across + down - 2, (across - 1) * (down - 1)
    vmem = pl.BlockSpec(memory_space=pltpu.VMEM)
    hbm = pl.BlockSpec(memory_space=pl.ANY)
    return pl.pallas_call(
        layer_kernel,
        out_shape=jax.ShapeDtypeStruct((row_count, cols), bf16),
        in_specs=[vmem] * 16 + [hbm] * 4,
        out_specs=vmem,
        scratch_shapes=[
            pltpu.VMEM((row_count, cols), f32),
            pltpu.VMEM((row_count, 2 * head_count), f32),
            pltpu.VMEM((2 * head_count, row_count), f32),
            pltpu.VMEM(query_small.shape, bf16),
            pltpu.VMEM(query_large.shape, bf16),
            pltpu.VMEM((2 * head_count, row_count, value_size), f32),
            pltpu.VMEM((pieces, size_a, value_size), f32),
            pltpu.VMEM((pieces, 1, value_size), f32),
            pltpu.VMEM((pieces, size_a, value_size), bf16),
            pltpu.VMEM((pieces, size_a, value_size), bf16),
            pltpu.VMEM((n_tp, 2, row_count, values.shape[2]), bf16),
            pltpu.VMEM((n_sp,) + out_weight.shape, bf16),
            pltpu.VMEM((row_count, cols), f32),
            pltpu.VMEM((width, units), bf16),
            pltpu.VMEM((width, units), bf16),
            pltpu.VMEM(expert_down.shape[1:], bf16),
            pltpu.VMEM((n_tp, 8, row_count), f32),
            pltpu.VMEM((slots, cols), bf16),
            pltpu.VMEM((n_tp, slots, cols), bf16),
            pltpu.VMEM((n_tp, slots, units), bf16),
            pltpu.VMEM((2, row_count, values.shape[2]), bf16),
            pltpu.VMEM((row_count, cols), bf16),
            pltpu.VMEM((row_count, cols), bf16),
            pltpu.VMEM((slots, cols), bf16),
            pltpu.VMEM((slots, cols), bf16),
            pltpu.VMEM((slots // GROUPS, units), f32),
            pltpu.VMEM((slots // GROUPS, units), f32),
            pltpu.VMEM((slots // GROUPS, cols), f32),
            dma((4,)),
            dma((pieces,)),
            dma((pieces,)),
            dma((2, n_tp)),
            dma((2, n_tp)),
            dma((n_sp,)),
            dma((n_sp,)),
            dma((n_sp,)),
            dma((2,)),
            dma((2,)),
            dma((n_tp,)),
            dma((n_tp,)),
            dma((n_sp,)),
            dma((n_sp,)),
            dma((GROUPS, straights)),
            dma((GROUPS, n_tp)),
            dma((GROUPS, 2, relays)),
            dma((GROUPS, n_tp, 2)),
            dma((GROUPS, straights)),
            dma((GROUPS, n_tp)),
            dma((GROUPS, 2, relays)),
            dma((GROUPS, n_tp, 2)),
            dma((n_sp,)),
            dma((n_sp,)),
        ],
        compiler_params=pltpu.CompilerParams(
            collective_id=0, has_side_effects=True, vmem_limit_bytes=58 * 2**20
        ),
    )(
        residual,
        query_small,
        key_narrow_group,
        query_large,
        key_large,
        values,
        gates,
        turn_a,
        start_a,
        turn_b,
        start_b,
        jnp.transpose(log_decay, (1, 2, 0)).reshape(2 * head_count, row_count),
        head_gain,
        norm_gain[None, :],
        routes.T,
        route_weight.T,
        out_weight,
        expert_gate,
        expert_up,
        expert_down,
    )


def solution(mesh):
    placed = (
        P("sp", "tp"),
        P("sp", "tp"),
        P("sp", "tp"),
        P("sp", "tp"),
        P("sp", "tp"),
        P("sp", None, "tp"),
        P("sp", None, "tp"),
        P("sp", None, "tp"),
        P(None, "tp"),
        P(None, "sp", "tp"),
        P("tp"),
        P("sp", None),
        P("sp", None),
        P("sp", None, "tp"),
        P("sp", None, "tp"),
        P("sp", None, "tp"),
    )
    return jax.shard_map(
        per_device, mesh=mesh, in_specs=placed, out_specs=P("sp", "tp"), check_vma=False
    )
```

```python
import jax
import jax.numpy as jnp
import numpy as np
from jax import lax
from jax.experimental import pallas as pl
from jax.experimental.pallas import tpu as pltpu
from jax.sharding import PartitionSpec as P

MESH = pl.DeviceIdType.MESH


EPS = 1e-06
THETA = 10000.0


def greet(axes):
    barrier = pltpu.get_barrier_semaphore()
    total = 0
    for axis in axes:
        count, me = lax.axis_size(axis), lax.axis_index(axis)

        def signal(k, _, axis=axis, count=count, me=me):
            pl.semaphore_signal(
                barrier, inc=1, device_id={axis: (me + k) % count}, device_id_type=MESH
            )
            return 0

        lax.fori_loop(1, count, signal, 0)
        total += count - 1
    pl.semaphore_wait(barrier, total)


def remote(source, target, send_sem, recv_sem, axis, index):
    return pltpu.make_async_remote_copy(
        src_ref=source,
        dst_ref=target,
        send_sem=send_sem,
        recv_sem=recv_sem,
        device_id={axis: index},
        device_id_type=MESH,
    )


GROUPS = 8


def grid_of(count):
    across = max(k for k in range(1, count + 1) if count % k == 0 and k * k <= count)
    return across, count // across


BETWEEN = ((2, 4, 5, 6, 7, 3), (4, 0, 1, 6, 7, 5), (2, 6, 7, 0, 1, 3), (4, 2, 3, 0, 1, 5))
ORDER = tuple((k,) + BETWEEN[k // 2] + (k ^ 1,) for k in range(GROUPS))
SENDS = (
    ((1, -2), (2, 3), (3, 4)),
    ((1, -2), (2, 3), (3, 4)),
    ((0, -2), (2, -2), (3, 2)),
    ((3, 3), (0, 4), (2, 5)),
    ((1, -2), (3, -1), (0, -1)),
    ((0, -1), (1, 4), (3, 5)),
    ((2, -2), (1, -1), (0, 2)),
    ((2, -2), (1, -1), (0, 2)),
)


def turned(block, cosine, sine):
    half = block.shape[1] // 2
    if half % 128:
        swapped = pltpu.roll(block, half, axis=1)
    else:
        swapped = jnp.concatenate([block[:, half:], block[:, :half]], axis=1)
    return block * cosine + swapped * sine


STAGED = 16


def layer_kernel(*refs):
    sources, refs = refs[:STAGED], refs[STAGED:]
    weights_and_out, refs = refs[:5], refs[5:]
    places, load_sem, refs = refs[:STAGED], refs[STAGED], refs[STAGED + 1 :]
    staged = [
        pltpu.make_async_copy(source, place, load_sem.at[i])
        for i, (source, place) in enumerate(zip(sources, places, strict=True))
    ]
    layer(staged, *places, *weights_and_out, *refs)


def layer(
    staged,
    residual_ref,
    query_a_ref,
    key_a_ref,
    query_b_ref,
    key_b_ref,
    values_ref,
    gates_ref,
    turn_a_ref,
    start_a_ref,
    turn_b_ref,
    start_b_ref,
    decay_ref,
    head_gain_ref,
    gain_ref,
    routes_ref,
    route_weight_ref,
    weight_hbm,
    gate_hbm,
    up_hbm,
    down_hbm,
    out_ref,
    picks,
    select,
    shares,
    stream_ref,
    cumul_ref,
    cumul_rows_ref,
    rot_queries_a,
    rot_queries_b,
    within,
    update,
    fall,
    held,
    departing,
    heads,
    w_out,
    mix,
    w_gate,
    w_up,
    w_down,
    squares,
    outgoing,
    arrived,
    hidden,
    scales_out,
    scales,
    far_heads,
    far_out,
    far_in,
    result,
    returned,
    acc_a,
    acc_b,
    acc_c,
    load_sem,
    chain_send,
    chain_recv,
    heads_send,
    heads_recv,
    w_line_send,
    w_pair_send,
    w_recv,
    far_send,
    far_recv,
    sq_send,
    sq_recv,
    disp_send,
    disp_recv,
    scale_send,
    scale_recv,
    fwd_send,
    fwd_recv,
    fwd_relay_send,
    fwd_relay_recv,
    hid_send,
    hid_recv,
    hid_relay_send,
    hid_relay_recv,
    ret_send,
    ret_recv,
):
    n_sp, n_tp = lax.axis_size("sp"), lax.axis_size("tp")
    s, t = lax.axis_index("sp"), lax.axis_index("tp")
    bf16, f32 = jnp.bfloat16, jnp.float32
    per_group = n_sp // GROUPS
    across, down = grid_of(n_tp)
    x, y = t % across, t // across
    cap = outgoing.shape[0] // n_sp
    cols = stream_ref.shape[1]
    units = w_gate.shape[1]
    count = stream_ref.shape[0]
    chips = n_sp // 2
    z, core = s // 2, s % 2
    loads = [
        pltpu.make_async_copy(source.at[0], target, load_sem.at[i])
        for i, (source, target) in enumerate(
            ((gate_hbm, w_gate), (up_hbm, w_up), (down_hbm, w_down))
        )
    ]
    own_load = pltpu.make_async_copy(weight_hbm, w_out.at[s], load_sem.at[3])
    own_load.start()
    for load in staged:
        load.start()
    for load in loads:
        load.start()
    with jax.named_scope("greet"):
        greet(("sp", "tp"))

    partner = s + 1 - 2 * core
    ahead = s + 2 - 4 * core
    has_ahead = jnp.where(core == 0, z < chips - 1, z > 0)

    wide = cols // 2

    def half(h):
        return pl.ds(h * wide, wide)

    def along_line(b, h):
        block = w_out.at[b, :, :, half(h)]
        return remote(block, block, w_line_send.at[h, b], w_recv.at[h, b], "sp", ahead)

    def to_partner(b, h):
        block = w_out.at[b, :, :, half(h)]
        return remote(block, block, w_pair_send.at[h, b], w_recv.at[h, b], "sp", partner)

    reach = chips - 2

    def pass_on(b, h, j):
        @pl.when(has_ahead & (j < reach))
        def _():
            along_line(b, h).start()

    with jax.named_scope("own"):
        own_load.wait()
    for h in range(2):
        to_partner(s, h).start()
        pass_on(s, h, 0)
    for load in staged:
        load.wait()

    def chip_behind(j):
        return z + (2 * core - 1) * j

    def serve(j, h, i):
        chip = chip_behind(j)

        @pl.when((chip >= 0) & (chip < chips))
        def _():
            b = chip * 2 + i
            along_line(b, h).wait_recv()
            to_partner(b, h).start()
            if h == 0:
                pass_on(b, h, j)

    def serve_right(j):
        for i in range(2):
            serve(j, 1, i)
        chip = chip_behind(j)

        @pl.when((chip >= 0) & (chip < chips) & has_ahead & (j < reach))
        def _():
            for i in range(2):
                along_line(chip * 2 + i, 0).wait_send()
                along_line(chip * 2 + i, 1).start()

    head_count = decay_ref.shape[0] // 2
    groups = (
        (query_a_ref, key_a_ref, turn_a_ref, start_a_ref, rot_queries_a),
        (query_b_ref, key_b_ref, turn_b_ref, start_b_ref, rot_queries_b),
    )
    size_a = query_a_ref.shape[1] // head_count
    dv = values_ref.shape[2] // head_count
    rows_i = lax.broadcasted_iota(jnp.int32, (count, count), 0)
    rows_j = lax.broadcasted_iota(jnp.int32, (count, count), 1)
    causal = rows_i >= rows_j
    exact = lax.Precision.HIGHEST
    cumul_rows_ref[...] = jnp.dot(
        decay_ref[...],
        jnp.where(rows_i <= rows_j, 1.0, 0.0),
        precision=exact,
        preferred_element_type=f32,
    )
    cumul_ref[...] = lax.dot_general(
        jnp.where(causal, 1.0, 0.0),
        decay_ref[...],
        (((1,), (1,)), ((), ())),
        precision=exact,
        preferred_element_type=f32,
    )

    def hop(c):
        return remote(
            departing.at[c], held.at[c], chain_send.at[c], chain_recv.at[c], "sp", (s + 1) % n_sp
        )

    pieces_of = []
    total_pieces = 0
    for g, (query_ref, key_ref, turn_ref, start_ref, rot_ref) in enumerate(groups):
        size = query_ref.shape[1] // head_count
        cos_start, sin_start = start_ref[0, pl.ds(s, 1), :], start_ref[1, pl.ds(s, 1), :]
        cosine = cos_start * turn_ref[0] - sin_start * turn_ref[1]
        sine = sin_start * turn_ref[0] + cos_start * turn_ref[1]
        for h in range(head_count):
            i = g * head_count + h
            lanes = slice(h * size, (h + 1) * size)
            rot_q = turned(query_ref[:, lanes].astype(f32), cosine, sine).astype(bf16)
            rot_k = (turned(key_ref[:, lanes].astype(f32), cosine, sine) * size ** (-0.5)).astype(
                bf16
            )
            rot_ref[:, lanes] = rot_q
            column, row = cumul_ref[:, i : i + 1], cumul_rows_ref[i : i + 1, :]
            scores = lax.dot_general(
                rot_q, rot_k, (((1,), (1,)), ((), ())), preferred_element_type=f32
            )
            spread = column - row
            weight = jnp.where(causal, jnp.exp(jnp.where(causal, spread, 0.0)), 0.0)
            value = values_ref[:, g, h * dv : (h + 1) * dv]
            within[i] = jnp.dot(
                (scores * weight).astype(bf16), value, preferred_element_type=f32
            )
            last = cumul_ref[count - 1 : count, i : i + 1]
            carried = (rot_k.astype(f32) * jnp.exp(last - column)).astype(bf16)
            grown = lax.dot_general(
                carried, value, (((0,), (0,)), ((), ())), preferred_element_type=f32
            )
            mine = []
            for c in range(size // size_a):
                update[total_pieces] = grown[c * size_a : (c + 1) * size_a]
                fall[total_pieces] = jnp.broadcast_to(jnp.exp(last), (1, dv))
                mine.append(total_pieces)
                total_pieces += 1
            pieces_of.append(mine)

    for h in range(2):
        to_partner(partner, h).wait_recv()
        pass_on(partner, h, 0)

    def step(c, _):
        @pl.when(s == 0)
        def _():
            held[c] = jnp.zeros(held.shape[1:], held.dtype)

        @pl.when(s > 0)
        def _():
            hop(c).wait_recv()

        @pl.when(s < n_sp - 1)
        def _():
            departing[c] = (fall[c] * held[c].astype(f32) + update[c]).astype(bf16)
            hop(c).start()

        return 0

    with jax.named_scope("chain"):
        lax.fori_loop(0, total_pieces, step, 0)

    with jax.named_scope("serve0"):
        serve(1, 0, 0)

    def heads_copy(g, k, source):
        block = heads.at[source, g]
        return remote(
            block, block, heads_send.at[g, k], heads_recv.at[g, source], "tp", (t + k) % n_tp
        )

    for g, (query_ref, _, _, _, rot_ref) in enumerate(groups):
        size = query_ref.shape[1] // head_count
        for h in range(head_count):
            i = g * head_count + h
            retained = within[i]
            cross = jnp.zeros((count, dv), f32)
            for c, piece in enumerate(pieces_of[i]):
                lanes = slice(h * size + c * size_a, h * size + (c + 1) * size_a)
                cross = cross + jnp.dot(rot_ref[:, lanes], held[piece], preferred_element_type=f32)
            retained = retained + cross * jnp.exp(cumul_ref[:, i : i + 1])
            scaled = retained * lax.rsqrt(
                jnp.mean(retained * retained, axis=1, keepdims=True) + EPS
            )
            lanes = slice(h * dv, (h + 1) * dv)
            gated = jax.nn.silu(gates_ref[:, g, lanes].astype(f32))
            heads[t, g, :, lanes] = (scaled * head_gain_ref[g : g + 1, lanes] * gated).astype(bf16)

        def heads_start(k, _, g=g):
            heads_copy(g, k, t).start()
            return 0

        lax.fori_loop(1, n_tp, heads_start, 0)

    with jax.named_scope("serve1"):
        serve(1, 0, 1)
    for g in range(2):

        def heads_wait(k, _, g=g):
            heads_copy(g, k, (t + k) % n_tp).wait_recv()
            return 0

        with jax.named_scope("headswait"):
            lax.fori_loop(1, n_tp, heads_wait, 0)

    at_low, at_high = z == 0, z == chips - 1
    near_low, near_high = z == 1, z == chips - 2

    def far_pair(low, shift, action):
        @pl.when(low)
        def _():
            action(shift)

    def ask(shift):
        return remote(
            heads.at[chips - 1 - z], far_heads, far_send.at[0], far_recv.at[0], "sp", s + shift
        )

    def answer(shift, h):
        return remote(
            far_out.at[:, half(h)],
            far_in.at[:, half(h)],
            far_send.at[1 + h],
            far_recv.at[1 + h],
            "sp",
            s + shift,
        )

    far_pair(at_low, 2, lambda shift: ask(shift).start())
    far_pair(at_high, -2, lambda shift: ask(shift).start())

    held_rows = w_out.shape[2]
    ratio = n_sp // n_tp

    def project_lanes(b, h, lanes):
        part = jnp.dot(
            heads[b // ratio, 0, :, lanes], w_out[b, 0, :, half(h)], preferred_element_type=f32
        )
        part += jnp.dot(
            heads[b // ratio, 1, :, lanes], w_out[b, 1, :, half(h)], preferred_element_type=f32
        )
        mix[:, half(h)] += part

    def project(b, h):
        if held_rows % 128 == 0:
            project_lanes(
                b, h, pl.ds(pl.multiple_of((b % ratio) * held_rows, held_rows), held_rows)
            )
            return
        for r in range(ratio):

            @pl.when(b % ratio == r)
            def _(r=r):
                project_lanes(b, h, slice(r * held_rows, (r + 1) * held_rows))

    def project_chips(j, h):
        chip = chip_behind(j)

        @pl.when((chip >= 0) & (chip < chips))
        def _():
            for i in range(2):
                project(chip * 2 + i, h)

        other = z - (2 * core - 1) * j

        @pl.when((other >= 0) & (other < chips))
        def _():
            for i in range(2):
                to_partner(other * 2 + i, h).wait_recv()
                project(other * 2 + i, h)

    def project_edge(shift, h):
        far = chips - 1 if shift < 0 else 0
        part = jnp.zeros((count, wide), f32)
        for i in range(2):
            lanes = slice(i * held_rows, (i + 1) * held_rows)
            for g in range(2):
                part += jnp.dot(
                    far_heads[g, :, lanes],
                    w_out[2 * far + i, g, :, half(h)],
                    preferred_element_type=f32,
                )
        far_out[:, half(h)] = part.astype(bf16)
        answer(shift, h).start()

    def add_edge(shift):
        for h in range(2):
            answer(shift, h).wait_recv()
        mix[...] += far_in[...].astype(f32)

    def rows_of(p):
        return pl.ds(pl.multiple_of(p * cap, cap), cap)

    eighth, quarter = s // per_group, s // (n_sp // 4)

    def group_base(g):
        base = ORDER[0][g]
        for k in range(1, GROUPS):
            base = jnp.where(eighth == k, ORDER[k][g], base)
        return base * per_group

    def group_rows(g, part=None):
        size = per_group * cap
        start = pl.multiple_of(group_base(g) * cap, size)
        if part is None:
            return pl.ds(start, size)
        return pl.ds(pl.multiple_of(start + part * (size // 2), size // 2), size // 2)

    def square_copy(k, source):
        block, other = squares.at[source], (t + k) % n_tp
        return remote(block, block, sq_send.at[k], sq_recv.at[source], "tp", other)

    def dispatch(p, q):
        return remote(
            outgoing.at[rows_of(p)],
            arrived.at[t, rows_of(q)],
            disp_send.at[p],
            disp_recv.at[q],
            "sp",
            p,
        )

    def members(g, action):
        def body(j, _):
            action(group_base(g) + j)
            return 0

        lax.fori_loop(0, per_group, body, 0)

    def others(g, action):
        def guarded(p):
            @pl.when(p != s)
            def _():
                action(p)

        members(g, guarded)

    def choose():
        numbers = lax.broadcasted_iota(jnp.int32, (n_sp, count), 0)
        named = [numbers == routes_ref[k : k + 1, :] for k in range(2)]
        counted = [jnp.where(mask, 1.0, 0.0).astype(bf16) for mask in named]
        earlier = jnp.where(rows_i < rows_j, 1.0, 0.0).astype(bf16)
        before = jnp.dot(counted[0] + counted[1], earlier, preferred_element_type=f32)
        down_slots = lax.broadcasted_iota(jnp.int32, (outgoing.shape[0], count), 0).astype(f32)
        along_slots = lax.broadcasted_iota(jnp.int32, (count, outgoing.shape[0]), 1).astype(f32)
        chosen = jnp.zeros((outgoing.shape[0], count), f32)
        for c in range(2):
            slot = jnp.sum(jnp.where(named[c], before, 0.0), axis=0, keepdims=True)
            target = (routes_ref[c : c + 1, :] * cap).astype(f32) + slot
            chosen = chosen + jnp.where(down_slots == target, 1.0, 0.0)
            column = jnp.broadcast_to(target, (count, count)).T[:, 0:1]
            picks[c] = jnp.where(along_slots == column, 1.0, 0.0).astype(bf16)
            shares[c] = jnp.broadcast_to(route_weight_ref[c : c + 1, :], (count, count)).T
        select[...] = chosen.astype(bf16)

    def square_start(k, _):
        square_copy(k, t).start()
        return 0

    def square_wait(k, _):
        square_copy(k, (t + k) % n_tp).wait()
        return 0

    def finish_rows():
        stream = residual_ref[...].astype(f32) + mix[...].astype(bf16).astype(f32)
        stream_ref[...] = stream
        own = jnp.sum(stream * stream, axis=1, keepdims=True)
        squares[t] = jnp.broadcast_to(own, (count, count)).T[0:8, :]
        lax.fori_loop(1, n_tp, square_start, 0)
        rows = (stream_ref[...] * gain_ref[...]).astype(bf16)
        outgoing[...] = jnp.dot(select[...], rows, preferred_element_type=f32).astype(bf16)
        arrived[t, rows_of(s)] = outgoing[rows_of(s)]

    def scale_copy(p, q):
        return remote(
            scales_out.at[rows_of(p)],
            scales.at[rows_of(q)],
            scale_send.at[p],
            scale_recv.at[q],
            "sp",
            p,
        )

    def finish_scale():
        lax.fori_loop(1, n_tp, square_wait, 0)
        total = squares[0]
        for p in range(1, n_tp):
            total = total + squares[p]
        scale = lax.rsqrt(total[0:1, :] / (cols * n_tp) + EPS)
        scale = jnp.broadcast_to(scale, (count, count)).T
        high = scale.astype(bf16)
        rest = scale - high.astype(f32)
        middle = rest.astype(bf16)
        low = (rest - middle.astype(f32)).astype(bf16)
        terms = jnp.where(
            rows_j == 0,
            high.astype(f32),
            jnp.where(
                rows_j == 1, middle.astype(f32), jnp.where(rows_j == 2, low.astype(f32), 0.0)
            ),
        ).astype(bf16)
        scales_out[...] = jnp.dot(select[...], terms, preferred_element_type=f32).astype(bf16)

        def send(p, _):
            @pl.when(p != s)
            def _():
                scale_copy(p, s).start()

            return 0

        lax.fori_loop(0, n_sp, send, 0)
        scales[rows_of(s)] = scales_out[rows_of(s)]

    def dispatch_to(q):
        def body(j, _):
            p = q * (n_sp // 4) + j

            @pl.when(p != s)
            def _():
                dispatch(p, s).start()

            return 0

        lax.fori_loop(0, n_sp // 4, body, 0)

    def dispatch_stage(moment):
        for k in range(GROUPS):
            for target, when in SENDS[k]:
                if when == moment:

                    @pl.when(eighth == k)
                    def _(target=target):
                        dispatch_to(target)

    lines = (
        [y * across + (x + k) % across for k in range(1, across)],
        [((y + k) % down) * across + x for k in range(1, down)],
    )
    direct = lines[0] + lines[1]

    def came_from(i):
        if i < len(lines[0]):
            return len(lines[0]) - 1 - i
        return len(direct) - 1 - (i - len(lines[0]))

    def straight(buffer, sems, g, i, source, rows, arriving=False):
        block = buffer.at[source, rows]
        there = came_from(i) if arriving else i
        return remote(block, block, sems[0].at[g, i], sems[1].at[g, there], "tp", direct[i])

    def relayed(buffer, sems, g, part, i, source, target):
        block = buffer.at[source, group_rows(g, part)]
        over = (source % across + across - target % across) % across - 1
        up = (source // across + down - target // across) % down - 1
        where = up * (across - 1) + over
        return remote(block, block, sems[2].at[g, part, i], sems[3].at[g, part, where], "tp", target)

    def relay(buffer, sems, g):
        for part in range(2):
            for k, source in enumerate(lines[part]):
                i = k if part == 0 else len(lines[0]) + k
                straight(buffer, sems, g, i, source, group_rows(g), True).wait_recv()
                for j, target in enumerate(lines[1 - part]):
                    relayed(
                        buffer, sems, g, part, k * len(lines[1 - part]) + j, source, target
                    ).start()

    def place_of(k):
        return ((y + k // across) % down) * across + (x + k % across) % across

    def wait_relayed(buffer, sems, g, k):
        @pl.when((k // across) * (k % across) > 0)
        def _():
            source = place_of(k)
            for part in range(2):
                relayed(buffer, sems, g, part, 0, source, t).wait_recv()

    def finish_sends(buffer, sems, g):
        for i in range(len(direct)):
            straight(buffer, sems, g, i, t, group_rows(g)).wait_send()
        for part in range(2):
            for i in range(len(lines[0]) * len(lines[1])):
                relayed(buffer, sems, g, part, i, place_of(across + 1), t).wait_send()

    arrived_sems = (fwd_send, fwd_recv, fwd_relay_send, fwd_relay_recv)
    hidden_sems = (hid_send, hid_recv, hid_relay_send, hid_relay_recv)

    def forward(g):
        def block(p):
            @pl.when(p != s)
            def _():
                dispatch(p, p).wait_recv()

            for i in range(len(direct)):
                straight(arrived, arrived_sems, g, i, t, rows_of(p)).start()

        with jax.named_scope("forward"):
            members(g, block)

    def through_units(g):
        acc_a[...] = jnp.zeros_like(acc_a)
        acc_b[...] = jnp.zeros_like(acc_b)

        def body(k, _):
            wait_relayed(arrived, arrived_sems, g, k)
            p = place_of(k)
            part = pl.ds(pl.multiple_of(p * cols, cols), cols)
            rows = arrived[p, group_rows(g)]
            acc_a[...] += jnp.dot(rows, w_gate[part, :], preferred_element_type=f32)
            acc_b[...] += jnp.dot(rows, w_up[part, :], preferred_element_type=f32)
            return 0

        with jax.named_scope("units"):
            lax.fori_loop(0, n_tp, body, 0)
        others(g, lambda p: scale_copy(p, p).wait_recv())
        terms = scales[group_rows(g)].astype(f32)
        scale = terms[:, 0:1] + (terms[:, 1:2] + terms[:, 2:3])
        hidden[t, group_rows(g)] = (
            jax.nn.silu(acc_a[...] * scale) * (acc_b[...] * scale)
        ).astype(bf16)
        for i in range(len(direct)):
            straight(hidden, hidden_sems, g, i, t, group_rows(g)).start()

    def give_back(p, q):
        return remote(
            result.at[rows_of(p)], returned.at[rows_of(q)], ret_send.at[p], ret_recv.at[q], "sp", p
        )

    def through_down(g):
        acc_c[...] = jnp.zeros_like(acc_c)

        def body(k, _):
            wait_relayed(hidden, hidden_sems, g, k)
            p = place_of(k)
            part = pl.ds(pl.multiple_of(p * units, units), units)
            acc_c[...] += jnp.dot(
                hidden[p, group_rows(g)], w_down[part, :], preferred_element_type=f32
            )
            return 0

        with jax.named_scope("down"):
            lax.fori_loop(0, n_tp, body, 0)
        result[group_rows(g)] = acc_c[...].astype(bf16)
        others(g, lambda p: give_back(p, s).start())

    def relay_rows(g):
        with jax.named_scope("relay_rows"):
            relay(arrived, arrived_sems, g)

    def relay_hidden(g):
        with jax.named_scope("relay_hidden"):
            relay(hidden, hidden_sems, g)

    mix[...] = jnp.zeros_like(mix)
    choose()
    with jax.named_scope("right"):
        serve_right(1)
    with jax.named_scope("proj1"):
        for h in range(2):
            for i in range(2):
                project(z * 2 + i, h)
            project_chips(1, h)

    def project_far(j, _):
        for h in range(2):
            if h == 0:
                for i in range(2):
                    serve(j, 0, i)
            else:
                serve_right(j)
            project_chips(j, h)
        return 0

    lax.fori_loop(2, reach, project_far, 0)
    far_pair(near_low, -2, lambda shift: ask(shift).wait_recv())
    far_pair(near_high, 2, lambda shift: ask(shift).wait_recv())
    for h in range(2):
        with jax.named_scope("far"):
            for i in range(2):
                serve(reach, h, i)
            project_chips(reach, h)
        far_pair(near_low, -2, lambda shift, h=h: project_edge(shift, h))
        far_pair(near_high, 2, lambda shift, h=h: project_edge(shift, h))
    with jax.named_scope("edge"):
        far_pair(at_low, 2, add_edge)
        far_pair(at_high, -2, add_edge)
    with jax.named_scope("finish"):
        finish_rows()
    dispatch_to(quarter)
    dispatch_stage(-2)
    forward(0)
    with jax.named_scope("scale"):
        finish_scale()
    for load in loads:
        load.wait()
    dispatch_stage(-1)

    def early_sends():
        @pl.when(s < n_sp - 1)
        def _():
            def gone(c, _):
                hop(c).wait_send()
                return 0

            lax.fori_loop(0, total_pieces, gone, 0)

        for g in range(2):

            def heads_gone(k, _, g=g):
                heads_copy(g, k, t).wait_send()
                return 0

            lax.fori_loop(1, n_tp, heads_gone, 0)

        def passed(j, _):
            chip = chip_behind(j)

            @pl.when((chip >= 0) & (chip < chips))
            def _():
                for i in range(2):
                    b = chip * 2 + i

                    @pl.when(has_ahead & (j < reach))
                    def _():
                        @pl.when(j == 0)
                        def _():
                            along_line(b, 0).wait_send()

                        along_line(b, 1).wait_send()

                    @pl.when((b == s) | (j > 0))
                    def _():
                        for h in range(2):
                            to_partner(b, h).wait_send()

            return 0

        lax.fori_loop(0, reach + 1, passed, 0)
        far_pair(at_low, 2, lambda shift: ask(shift).wait_send())
        far_pair(at_high, -2, lambda shift: ask(shift).wait_send())
        for h in range(2):
            far_pair(near_low, -2, lambda shift, h=h: answer(shift, h).wait_send())
            far_pair(near_high, 2, lambda shift, h=h: answer(shift, h).wait_send())

    for step in range(GROUPS):
        if step > 0:
            dispatch_stage(step)
            forward(step)
            relay_rows(step - 1)
        if step >= 2:
            through_units(step - 2)
        if step >= 3:
            relay_hidden(step - 3)
        if step == 3:
            early_sends()
        if step >= 4:
            through_down(step - 4)
            finish_sends(arrived, arrived_sems, step - 4)
    last = GROUPS - 1
    relay_rows(last)
    through_units(last - 1)
    relay_hidden(last - 2)
    through_units(last)
    relay_hidden(last - 1)
    for g in range(last - 3, last - 1):
        through_down(g)
    relay_hidden(last)
    for g in range(last - 1, last + 1):
        through_down(g)
    for g in range(GROUPS):
        others(g, lambda p: dispatch(p, s).wait_send())
        others(g, lambda p: scale_copy(p, s).wait_send())
        if g >= last - 3:
            finish_sends(arrived, arrived_sems, g)
        finish_sends(hidden, hidden_sems, g)

    returned[rows_of(s)] = result[rows_of(s)]
    with jax.named_scope("back"):
        for g in range(GROUPS):
            others(g, lambda p: give_back(p, p).wait_recv())
    combine_scope = jax.named_scope("combine")
    combine_scope.__enter__()
    total = stream_ref[...]
    for c in range(2):
        pick = jnp.dot(picks[c], returned[...], preferred_element_type=f32)
        total = total + shares[c][:, 0:1] * pick
    out_ref[...] = total.astype(bf16)
    combine_scope.__exit__(None, None, None)

    with jax.named_scope("sent"):
        for g in range(GROUPS):
            others(g, lambda p: give_back(p, s).wait_send())


def tables(rows, blocks, size):
    half = size // 2
    inverse = np.power(THETA, -np.arange(half) * 2.0 / size)
    inverse = np.concatenate([inverse, inverse])
    sign = np.where(np.arange(size) < half, -1.0, 1.0)

    def at(positions):
        angles = positions[:, None] * inverse[None, :]
        return jnp.asarray(np.stack([np.cos(angles), np.sin(angles) * sign]), jnp.float32)

    return at(np.arange(rows)), at(np.arange(blocks) * rows)


def per_device(
    residual,
    query_small,
    key_narrow_group,
    query_large,
    key_large,
    values,
    gates,
    log_decay,
    head_gain,
    out_weight,
    norm_gain,
    routes,
    route_weight,
    expert_gate,
    expert_up,
    expert_down,
):
    n_sp, n_tp = lax.axis_size("sp"), lax.axis_size("tp")
    row_count, cols = residual.shape
    head_count = log_decay.shape[2]
    bf16, f32 = jnp.bfloat16, jnp.float32
    size_a, size_b = query_small.shape[1] // head_count, query_large.shape[1] // head_count
    turn_a, start_a = tables(row_count, n_sp, size_a)
    turn_b, start_b = tables(row_count, n_sp, size_b)
    slots = 4 * row_count
    pieces = head_count * (1 + size_b // size_a)
    value_size = values.shape[2] // head_count
    width, units = expert_gate.shape[1:]
    dma = pltpu.SemaphoreType.DMA
    across, down = grid_of(n_tp)
    straights, relays = across + down - 2, (across - 1) * (down - 1)
    vmem = pl.BlockSpec(memory_space=pltpu.VMEM)
    hbm = pl.BlockSpec(memory_space=pl.ANY)
    inputs = (
        residual,
        query_small,
        key_narrow_group,
        query_large,
        key_large,
        values,
        gates,
        turn_a,
        start_a,
        turn_b,
        start_b,
        jnp.transpose(log_decay, (1, 2, 0)).reshape(2 * head_count, row_count),
        head_gain,
        norm_gain[None, :],
        routes.T,
        route_weight.T,
    )
    return pl.pallas_call(
        layer_kernel,
        out_shape=jax.ShapeDtypeStruct((row_count, cols), bf16),
        in_specs=[hbm] * (STAGED + 4),
        out_specs=vmem,
        scratch_shapes=[pltpu.VMEM(a.shape, a.dtype) for a in inputs]
        + [
            dma((STAGED,)),
            pltpu.VMEM((2, row_count, slots), bf16),
            pltpu.VMEM((slots, row_count), bf16),
            pltpu.VMEM((2, row_count, row_count), f32),
            pltpu.VMEM((row_count, cols), f32),
            pltpu.VMEM((row_count, 2 * head_count), f32),
            pltpu.VMEM((2 * head_count, row_count), f32),
            pltpu.VMEM(query_small.shape, bf16),
            pltpu.VMEM(query_large.shape, bf16),
            pltpu.VMEM((2 * head_count, row_count, value_size), f32),
            pltpu.VMEM((pieces, size_a, value_size), f32),
            pltpu.VMEM((pieces, 1, value_size), f32),
            pltpu.VMEM((pieces, size_a, value_size), bf16),
            pltpu.VMEM((pieces, size_a, value_size), bf16),
            pltpu.VMEM((n_tp, 2, row_count, values.shape[2]), bf16),
            pltpu.VMEM((n_sp,) + out_weight.shape, bf16),
            pltpu.VMEM((row_count, cols), f32),
            pltpu.VMEM((width, units), bf16),
            pltpu.VMEM((width, units), bf16),
            pltpu.VMEM(expert_down.shape[1:], bf16),
            pltpu.VMEM((n_tp, 8, row_count), f32),
            pltpu.VMEM((slots, cols), bf16),
            pltpu.VMEM((n_tp, slots, cols), bf16),
            pltpu.VMEM((n_tp, slots, units), bf16),
            pltpu.VMEM((slots, 128), bf16),
            pltpu.VMEM((slots, 128), bf16),
            pltpu.VMEM((2, row_count, values.shape[2]), bf16),
            pltpu.VMEM((row_count, cols), bf16),
            pltpu.VMEM((row_count, cols), bf16),
            pltpu.VMEM((slots, cols), bf16),
            pltpu.VMEM((slots, cols), bf16),
            pltpu.VMEM((slots // GROUPS, units), f32),
            pltpu.VMEM((slots // GROUPS, units), f32),
            pltpu.VMEM((slots // GROUPS, cols), f32),
            dma((4,)),
            dma((pieces,)),
            dma((pieces,)),
            dma((2, n_tp)),
            dma((2, n_tp)),
            dma((2, n_sp)),
            dma((2, n_sp)),
            dma((2, n_sp)),
            dma((3,)),
            dma((3,)),
            dma((n_tp,)),
            dma((n_tp,)),
            dma((n_sp,)),
            dma((n_sp,)),
            dma((n_sp,)),
            dma((n_sp,)),
            dma((GROUPS, straights)),
            dma((GROUPS, straights)),
            dma((GROUPS, 2, relays)),
            dma((GROUPS, 2, relays)),
            dma((GROUPS, straights)),
            dma((GROUPS, straights)),
            dma((GROUPS, 2, relays)),
            dma((GROUPS, 2, relays)),
            dma((n_sp,)),
            dma((n_sp,)),
        ],
        compiler_params=pltpu.CompilerParams(
            collective_id=0, has_side_effects=True, vmem_limit_bytes=58 * 2**20
        ),
    )(*inputs, out_weight, expert_gate, expert_up, expert_down)


def solution(mesh):
    placed = (
        P("sp", "tp"),
        P("sp", "tp"),
        P("sp", "tp"),
        P("sp", "tp"),
        P("sp", "tp"),
        P("sp", None, "tp"),
        P("sp", None, "tp"),
        P("sp", None, "tp"),
        P(None, "tp"),
        P(None, "sp", "tp"),
        P("tp"),
        P("sp", None),
        P("sp", None),
        P("sp", None, "tp"),
        P("sp", None, "tp"),
        P("sp", None, "tp"),
    )
    return jax.shard_map(
        per_device, mesh=mesh, in_specs=placed, out_specs=P("sp", "tp"), check_vma=False
    )
```

```python
import jax
import jax.numpy as jnp
import numpy as np
from jax import lax
from jax.experimental import pallas as pl
from jax.experimental.pallas import tpu as pltpu
from jax.sharding import PartitionSpec as P

MESH = pl.DeviceIdType.MESH


EPS = 1e-06
THETA = 10000.0


def greet(axes):
    barrier = pltpu.get_barrier_semaphore()
    total = 0
    for axis in axes:
        count, me = lax.axis_size(axis), lax.axis_index(axis)

        def signal(k, _, axis=axis, count=count, me=me):
            pl.semaphore_signal(
                barrier, inc=1, device_id={axis: (me + k) % count}, device_id_type=MESH
            )
            return 0

        lax.fori_loop(1, count, signal, 0)
        total += count - 1
    pl.semaphore_wait(barrier, total)


def remote(source, target, send_sem, recv_sem, axis, index):
    return pltpu.make_async_remote_copy(
        src_ref=source,
        dst_ref=target,
        send_sem=send_sem,
        recv_sem=recv_sem,
        device_id={axis: index},
        device_id_type=MESH,
    )


GROUPS = 8


def grid_of(count):
    across = max(k for k in range(1, count + 1) if count % k == 0 and k * k <= count)
    return across, count // across


BETWEEN = ((2, 4, 5, 6, 7, 3), (4, 0, 1, 6, 7, 5), (2, 6, 7, 0, 1, 3), (4, 2, 3, 0, 1, 5))
ORDER = tuple((k,) + BETWEEN[k // 2] + (k ^ 1,) for k in range(GROUPS))
SENDS = (
    ((1, -2), (2, 3), (3, 4)),
    ((1, -2), (2, 3), (3, 4)),
    ((0, -2), (2, -2), (3, 2)),
    ((3, 3), (0, 4), (2, 5)),
    ((1, -2), (3, -1), (0, -1)),
    ((0, -1), (1, 4), (3, 5)),
    ((2, -2), (1, -1), (0, 2)),
    ((2, -2), (1, -1), (0, 2)),
)


def turned(block, cosine, sine):
    half = block.shape[1] // 2
    if half % 128:
        swapped = pltpu.roll(block, half, axis=1)
    else:
        swapped = jnp.concatenate([block[:, half:], block[:, :half]], axis=1)
    return block * cosine + swapped * sine


STAGED = 16


def layer_kernel(*refs):
    sources, refs = refs[:STAGED], refs[STAGED:]
    weights_and_out, refs = refs[:5], refs[5:]
    places, load_sem, refs = refs[:STAGED], refs[STAGED], refs[STAGED + 1 :]
    staged = [
        pltpu.make_async_copy(source, place, load_sem.at[i])
        for i, (source, place) in enumerate(zip(sources, places, strict=True))
    ]
    layer(staged, *places, *weights_and_out, *refs)


def layer(
    staged,
    residual_ref,
    query_a_ref,
    key_a_ref,
    query_b_ref,
    key_b_ref,
    values_ref,
    gates_ref,
    turn_a_ref,
    start_a_ref,
    turn_b_ref,
    start_b_ref,
    decay_ref,
    head_gain_ref,
    gain_ref,
    routes_ref,
    route_weight_ref,
    weight_hbm,
    gate_hbm,
    up_hbm,
    down_hbm,
    out_ref,
    picks,
    select,
    shares,
    stream_ref,
    cumul_ref,
    cumul_rows_ref,
    rot_queries_a,
    rot_queries_b,
    within,
    update,
    fall,
    held,
    departing,
    heads,
    w_out,
    mix,
    w_gate,
    w_up,
    w_down,
    squares,
    outgoing,
    arrived,
    hidden,
    scales_out,
    scales,
    far_heads,
    far_out,
    far_in,
    result,
    returned,
    acc_a,
    acc_b,
    acc_c,
    load_sem,
    chain_send,
    chain_recv,
    heads_send,
    heads_recv,
    w_line_send,
    w_pair_send,
    w_recv,
    far_send,
    far_recv,
    sq_send,
    sq_recv,
    disp_send,
    disp_recv,
    scale_send,
    scale_recv,
    fwd_send,
    fwd_recv,
    fwd_relay_send,
    fwd_relay_recv,
    hid_send,
    hid_recv,
    hid_relay_send,
    hid_relay_recv,
    ret_send,
    ret_recv,
):
    n_sp, n_tp = lax.axis_size("sp"), lax.axis_size("tp")
    s, t = lax.axis_index("sp"), lax.axis_index("tp")
    bf16, f32 = jnp.bfloat16, jnp.float32
    per_group = n_sp // GROUPS
    across, down = grid_of(n_tp)
    x, y = t % across, t // across
    cap = outgoing.shape[0] // n_sp
    cols = stream_ref.shape[1]
    units = w_gate.shape[1]
    count = stream_ref.shape[0]
    chips = n_sp // 2
    z, core = s // 2, s % 2
    loads = [
        pltpu.make_async_copy(source.at[0], target, load_sem.at[i])
        for i, (source, target) in enumerate(
            ((gate_hbm, w_gate), (up_hbm, w_up), (down_hbm, w_down))
        )
    ]
    own_load = pltpu.make_async_copy(weight_hbm, w_out.at[s], load_sem.at[3])
    own_load.start()
    for load in staged:
        load.start()
    for load in loads:
        load.start()
    with jax.named_scope("greet"):
        greet(("sp", "tp"))

    partner = s + 1 - 2 * core
    ahead = s + 2 - 4 * core
    has_ahead = jnp.where(core == 0, z < chips - 1, z > 0)

    wide = cols // 2

    def half(h):
        return pl.ds(h * wide, wide)

    def along_line(b, h):
        block = w_out.at[b, :, :, half(h)]
        return remote(block, block, w_line_send.at[h, b], w_recv.at[h, b], "sp", ahead)

    def to_partner(b, h):
        block = w_out.at[b, :, :, half(h)]
        return remote(block, block, w_pair_send.at[h, b], w_recv.at[h, b], "sp", partner)

    reach = chips - 2

    def pass_on(b, h, j):
        @pl.when(has_ahead & (j < reach))
        def _():
            along_line(b, h).start()

    with jax.named_scope("own"):
        own_load.wait()
    for h in range(2):
        to_partner(s, h).start()
        pass_on(s, h, 0)
    for load in staged:
        load.wait()

    def chip_behind(j):
        return z + (2 * core - 1) * j

    def serve(j, h, i):
        chip = chip_behind(j)

        @pl.when((chip >= 0) & (chip < chips))
        def _():
            b = chip * 2 + i
            along_line(b, h).wait_recv()
            to_partner(b, h).start()
            if h == 0:
                pass_on(b, h, j)

    def serve_right(j):
        for i in range(2):
            serve(j, 1, i)
        chip = chip_behind(j)

        @pl.when((chip >= 0) & (chip < chips) & has_ahead & (j < reach))
        def _():
            for i in range(2):
                along_line(chip * 2 + i, 0).wait_send()
                along_line(chip * 2 + i, 1).start()

    head_count = decay_ref.shape[0] // 2
    groups = (
        (query_a_ref, key_a_ref, turn_a_ref, start_a_ref, rot_queries_a),
        (query_b_ref, key_b_ref, turn_b_ref, start_b_ref, rot_queries_b),
    )
    size_a = query_a_ref.shape[1] // head_count
    dv = values_ref.shape[2] // head_count
    rows_i = lax.broadcasted_iota(jnp.int32, (count, count), 0)
    rows_j = lax.broadcasted_iota(jnp.int32, (count, count), 1)
    causal = rows_i >= rows_j
    exact = lax.Precision.HIGHEST
    cumul_rows_ref[...] = jnp.dot(
        decay_ref[...],
        jnp.where(rows_i <= rows_j, 1.0, 0.0),
        precision=exact,
        preferred_element_type=f32,
    )
    cumul_ref[...] = lax.dot_general(
        jnp.where(causal, 1.0, 0.0),
        decay_ref[...],
        (((1,), (1,)), ((), ())),
        precision=exact,
        preferred_element_type=f32,
    )

    def hop(c):
        return remote(
            departing.at[c], held.at[c], chain_send.at[c], chain_recv.at[c], "sp", (s + 1) % n_sp
        )

    pieces_of = []
    total_pieces = 0
    for g, (query_ref, key_ref, turn_ref, start_ref, rot_ref) in enumerate(groups):
        size = query_ref.shape[1] // head_count
        cos_start, sin_start = start_ref[0, pl.ds(s, 1), :], start_ref[1, pl.ds(s, 1), :]
        cosine = cos_start * turn_ref[0] - sin_start * turn_ref[1]
        sine = sin_start * turn_ref[0] + cos_start * turn_ref[1]
        for h in range(head_count):
            i = g * head_count + h
            lanes = slice(h * size, (h + 1) * size)
            rot_q = turned(query_ref[:, lanes].astype(f32), cosine, sine).astype(bf16)
            rot_k = (turned(key_ref[:, lanes].astype(f32), cosine, sine) * size ** (-0.5)).astype(
                bf16
            )
            rot_ref[:, lanes] = rot_q
            column, row = cumul_ref[:, i : i + 1], cumul_rows_ref[i : i + 1, :]
            scores = lax.dot_general(
                rot_q, rot_k, (((1,), (1,)), ((), ())), preferred_element_type=f32
            )
            spread = column - row
            weight = jnp.where(causal, jnp.exp(jnp.where(causal, spread, 0.0)), 0.0)
            value = values_ref[:, g, h * dv : (h + 1) * dv]
            within[i] = jnp.dot(
                (scores * weight).astype(bf16), value, preferred_element_type=f32
            )
            last = cumul_ref[count - 1 : count, i : i + 1]
            carried = (rot_k.astype(f32) * jnp.exp(last - column)).astype(bf16)
            grown = lax.dot_general(
                carried, value, (((0,), (0,)), ((), ())), preferred_element_type=f32
            )
            mine = []
            for c in range(size // size_a):
                update[total_pieces] = grown[c * size_a : (c + 1) * size_a]
                fall[total_pieces] = jnp.broadcast_to(jnp.exp(last), (1, dv))
                mine.append(total_pieces)
                total_pieces += 1
            pieces_of.append(mine)

    for h in range(2):
        to_partner(partner, h).wait_recv()
        pass_on(partner, h, 0)

    def step(c, _):
        @pl.when(s == 0)
        def _():
            held[c] = jnp.zeros(held.shape[1:], held.dtype)

        @pl.when(s > 0)
        def _():
            hop(c).wait_recv()

        @pl.when(s < n_sp - 1)
        def _():
            departing[c] = (fall[c] * held[c].astype(f32) + update[c]).astype(bf16)
            hop(c).start()

        return 0

    with jax.named_scope("chain"):
        lax.fori_loop(0, total_pieces, step, 0)

    with jax.named_scope("serve0"):
        serve(1, 0, 0)

    def heads_copy(g, k, source):
        block = heads.at[source, g]
        return remote(
            block, block, heads_send.at[g, k], heads_recv.at[g, source], "tp", (t + k) % n_tp
        )

    for g, (query_ref, _, _, _, rot_ref) in enumerate(groups):
        size = query_ref.shape[1] // head_count
        for h in range(head_count):
            i = g * head_count + h
            retained = within[i]
            cross = jnp.zeros((count, dv), f32)
            for c, piece in enumerate(pieces_of[i]):
                lanes = slice(h * size + c * size_a, h * size + (c + 1) * size_a)
                cross = cross + jnp.dot(rot_ref[:, lanes], held[piece], preferred_element_type=f32)
            retained = retained + cross * jnp.exp(cumul_ref[:, i : i + 1])
            scaled = retained * lax.rsqrt(
                jnp.mean(retained * retained, axis=1, keepdims=True) + EPS
            )
            lanes = slice(h * dv, (h + 1) * dv)
            gated = jax.nn.silu(gates_ref[:, g, lanes].astype(f32))
            heads[t, g, :, lanes] = (scaled * head_gain_ref[g : g + 1, lanes] * gated).astype(bf16)

        def heads_start(k, _, g=g):
            heads_copy(g, k, t).start()
            return 0

        lax.fori_loop(1, n_tp, heads_start, 0)

    with jax.named_scope("serve1"):
        serve(1, 0, 1)
    for g in range(2):

        def heads_wait(k, _, g=g):
            heads_copy(g, k, (t + k) % n_tp).wait_recv()
            return 0

        with jax.named_scope("headswait"):
            lax.fori_loop(1, n_tp, heads_wait, 0)

    at_low, at_high = z == 0, z == chips - 1
    near_low, near_high = z == 1, z == chips - 2

    def far_pair(low, shift, action):
        @pl.when(low)
        def _():
            action(shift)

    def ask(shift):
        return remote(
            heads.at[chips - 1 - z], far_heads, far_send.at[0], far_recv.at[0], "sp", s + shift
        )

    def answer(shift, h):
        return remote(
            far_out.at[:, half(h)],
            far_in.at[:, half(h)],
            far_send.at[1 + h],
            far_recv.at[1 + h],
            "sp",
            s + shift,
        )

    far_pair(at_low, 2, lambda shift: ask(shift).start())
    far_pair(at_high, -2, lambda shift: ask(shift).start())

    held_rows = w_out.shape[2]
    ratio = n_sp // n_tp

    def project_lanes(b, h, lanes):
        part = jnp.dot(
            heads[b // ratio, 0, :, lanes], w_out[b, 0, :, half(h)], preferred_element_type=f32
        )
        part += jnp.dot(
            heads[b // ratio, 1, :, lanes], w_out[b, 1, :, half(h)], preferred_element_type=f32
        )
        mix[:, half(h)] += part

    def project(b, h):
        if held_rows % 128 == 0:
            project_lanes(
                b, h, pl.ds(pl.multiple_of((b % ratio) * held_rows, held_rows), held_rows)
            )
            return
        for r in range(ratio):

            @pl.when(b % ratio == r)
            def _(r=r):
                project_lanes(b, h, slice(r * held_rows, (r + 1) * held_rows))

    def project_chips(j, h):
        chip = chip_behind(j)

        @pl.when((chip >= 0) & (chip < chips))
        def _():
            for i in range(2):
                project(chip * 2 + i, h)

        other = z - (2 * core - 1) * j

        @pl.when((other >= 0) & (other < chips))
        def _():
            for i in range(2):
                to_partner(other * 2 + i, h).wait_recv()
                project(other * 2 + i, h)

    def project_edge(shift, h):
        far = chips - 1 if shift < 0 else 0
        part = jnp.zeros((count, wide), f32)
        for i in range(2):
            lanes = slice(i * held_rows, (i + 1) * held_rows)
            for g in range(2):
                part += jnp.dot(
                    far_heads[g, :, lanes],
                    w_out[2 * far + i, g, :, half(h)],
                    preferred_element_type=f32,
                )
        far_out[:, half(h)] = part.astype(bf16)
        answer(shift, h).start()

    def add_edge(shift):
        for h in range(2):
            answer(shift, h).wait_recv()
        mix[...] += far_in[...].astype(f32)

    def rows_of(p):
        return pl.ds(pl.multiple_of(p * cap, cap), cap)

    eighth, quarter = s // per_group, s // (n_sp // 4)

    def group_base(g):
        base = ORDER[0][g]
        for k in range(1, GROUPS):
            base = jnp.where(eighth == k, ORDER[k][g], base)
        return base * per_group

    def group_rows(g, part=None):
        size = per_group * cap
        start = pl.multiple_of(group_base(g) * cap, size)
        if part is None:
            return pl.ds(start, size)
        return pl.ds(pl.multiple_of(start + part * (size // 2), size // 2), size // 2)

    def square_copy(k, source):
        block, other = squares.at[source], (t + k) % n_tp
        return remote(block, block, sq_send.at[k], sq_recv.at[source], "tp", other)

    def dispatch(p, q):
        return remote(
            outgoing.at[rows_of(p)],
            arrived.at[t, rows_of(q)],
            disp_send.at[p],
            disp_recv.at[q],
            "sp",
            p,
        )

    def members(g, action):
        def body(j, _):
            action(group_base(g) + j)
            return 0

        lax.fori_loop(0, per_group, body, 0)

    def others(g, action):
        def guarded(p):
            @pl.when(p != s)
            def _():
                action(p)

        members(g, guarded)

    def choose():
        numbers = lax.broadcasted_iota(jnp.int32, (n_sp, count), 0)
        named = [numbers == routes_ref[k : k + 1, :] for k in range(2)]
        counted = [jnp.where(mask, 1.0, 0.0).astype(bf16) for mask in named]
        earlier = jnp.where(rows_i < rows_j, 1.0, 0.0).astype(bf16)
        before = jnp.dot(counted[0] + counted[1], earlier, preferred_element_type=f32)
        down_slots = lax.broadcasted_iota(jnp.int32, (outgoing.shape[0], count), 0).astype(f32)
        along_slots = lax.broadcasted_iota(jnp.int32, (count, outgoing.shape[0]), 1).astype(f32)
        chosen = jnp.zeros((outgoing.shape[0], count), f32)
        for c in range(2):
            slot = jnp.sum(jnp.where(named[c], before, 0.0), axis=0, keepdims=True)
            target = (routes_ref[c : c + 1, :] * cap).astype(f32) + slot
            chosen = chosen + jnp.where(down_slots == target, 1.0, 0.0)
            column = jnp.broadcast_to(target, (count, count)).T[:, 0:1]
            picks[c] = jnp.where(along_slots == column, 1.0, 0.0).astype(bf16)
            shares[c] = jnp.broadcast_to(route_weight_ref[c : c + 1, :], (count, count)).T
        select[...] = chosen.astype(bf16)

    def square_start(k, _):
        square_copy(k, t).start()
        return 0

    def square_wait(k, _):
        square_copy(k, (t + k) % n_tp).wait()
        return 0

    def finish_rows():
        stream = residual_ref[...].astype(f32) + mix[...].astype(bf16).astype(f32)
        stream_ref[...] = stream
        own = jnp.sum(stream * stream, axis=1, keepdims=True)
        squares[t] = jnp.broadcast_to(own, (count, count)).T[0:8, :]
        lax.fori_loop(1, n_tp, square_start, 0)
        rows = (stream_ref[...] * gain_ref[...]).astype(bf16)
        outgoing[...] = jnp.dot(select[...], rows, preferred_element_type=f32).astype(bf16)
        arrived[t, rows_of(s)] = outgoing[rows_of(s)]

    def scale_copy(p, q):
        return remote(
            scales_out.at[rows_of(p)],
            scales.at[rows_of(q)],
            scale_send.at[p],
            scale_recv.at[q],
            "sp",
            p,
        )

    def finish_scale():
        lax.fori_loop(1, n_tp, square_wait, 0)
        total = squares[0]
        for p in range(1, n_tp):
            total = total + squares[p]
        scale = lax.rsqrt(total[0:1, :] / (cols * n_tp) + EPS)
        scale = jnp.broadcast_to(scale, (count, count)).T
        high = scale.astype(bf16)
        rest = scale - high.astype(f32)
        middle = rest.astype(bf16)
        low = (rest - middle.astype(f32)).astype(bf16)
        terms = jnp.where(
            rows_j == 0,
            high.astype(f32),
            jnp.where(
                rows_j == 1, middle.astype(f32), jnp.where(rows_j == 2, low.astype(f32), 0.0)
            ),
        ).astype(bf16)
        scales_out[...] = jnp.dot(select[...], terms, preferred_element_type=f32).astype(bf16)

        def send(p, _):
            @pl.when(p != s)
            def _():
                scale_copy(p, s).start()

            return 0

        lax.fori_loop(0, n_sp, send, 0)
        scales[rows_of(s)] = scales_out[rows_of(s)]

    def dispatch_to(q):
        def body(j, _):
            p = q * (n_sp // 4) + j

            @pl.when(p != s)
            def _():
                dispatch(p, s).start()

            return 0

        lax.fori_loop(0, n_sp // 4, body, 0)

    def dispatch_stage(moment):
        for k in range(GROUPS):
            for target, when in SENDS[k]:
                if when == moment:

                    @pl.when(eighth == k)
                    def _(target=target):
                        dispatch_to(target)

    lines = (
        [y * across + (x + k) % across for k in range(1, across)],
        [((y + k) % down) * across + x for k in range(1, down)],
    )
    direct = lines[0] + lines[1]

    def came_from(i):
        if i < len(lines[0]):
            return len(lines[0]) - 1 - i
        return len(direct) - 1 - (i - len(lines[0]))

    def straight(buffer, sems, g, i, source, rows, arriving=False):
        block = buffer.at[source, rows]
        there = came_from(i) if arriving else i
        return remote(block, block, sems[0].at[g, i], sems[1].at[g, there], "tp", direct[i])

    def relayed(buffer, sems, g, part, i, source, target):
        block = buffer.at[source, group_rows(g, part)]
        over = (source % across + across - target % across) % across - 1
        up = (source // across + down - target // across) % down - 1
        where = up * (across - 1) + over
        return remote(block, block, sems[2].at[g, part, i], sems[3].at[g, part, where], "tp", target)

    def relay(buffer, sems, g):
        for part in range(2):
            for k, source in enumerate(lines[part]):
                i = k if part == 0 else len(lines[0]) + k
                straight(buffer, sems, g, i, source, group_rows(g), True).wait_recv()
                for j, target in enumerate(lines[1 - part]):
                    relayed(
                        buffer, sems, g, part, k * len(lines[1 - part]) + j, source, target
                    ).start()

    def place_of(k):
        return ((y + k // across) % down) * across + (x + k % across) % across

    def wait_relayed(buffer, sems, g, k):
        @pl.when((k // across) * (k % across) > 0)
        def _():
            source = place_of(k)
            for part in range(2):
                relayed(buffer, sems, g, part, 0, source, t).wait_recv()

    def finish_sends(buffer, sems, g):
        for i in range(len(direct)):
            straight(buffer, sems, g, i, t, group_rows(g)).wait_send()
        for part in range(2):
            for i in range(len(lines[0]) * len(lines[1])):
                relayed(buffer, sems, g, part, i, place_of(across + 1), t).wait_send()

    arrived_sems = (fwd_send, fwd_recv, fwd_relay_send, fwd_relay_recv)
    hidden_sems = (hid_send, hid_recv, hid_relay_send, hid_relay_recv)

    def forward(g):
        def block(p):
            @pl.when(p != s)
            def _():
                dispatch(p, p).wait_recv()

            for i in range(len(direct)):
                straight(arrived, arrived_sems, g, i, t, rows_of(p)).start()

        with jax.named_scope("forward"):
            members(g, block)

    def through_units(g):
        acc_a[...] = jnp.zeros_like(acc_a)
        acc_b[...] = jnp.zeros_like(acc_b)

        def body(k, _):
            wait_relayed(arrived, arrived_sems, g, k)
            p = place_of(k)
            part = pl.ds(pl.multiple_of(p * cols, cols), cols)
            rows = arrived[p, group_rows(g)]
            acc_a[...] += jnp.dot(rows, w_gate[part, :], preferred_element_type=f32)
            acc_b[...] += jnp.dot(rows, w_up[part, :], preferred_element_type=f32)
            return 0

        with jax.named_scope("units"):
            lax.fori_loop(0, n_tp, body, 0)
        others(g, lambda p: scale_copy(p, p).wait_recv())
        terms = scales[group_rows(g)].astype(f32)
        scale = terms[:, 0:1] + (terms[:, 1:2] + terms[:, 2:3])
        hidden[t, group_rows(g)] = (
            jax.nn.silu(acc_a[...] * scale) * (acc_b[...] * scale)
        ).astype(bf16)
        for i in range(len(direct)):
            straight(hidden, hidden_sems, g, i, t, group_rows(g)).start()

    def give_back(p, q):
        return remote(
            result.at[rows_of(p)], returned.at[rows_of(q)], ret_send.at[p], ret_recv.at[q], "sp", p
        )

    def through_down(g):
        acc_c[...] = jnp.zeros_like(acc_c)

        def body(k, _):
            wait_relayed(hidden, hidden_sems, g, k)
            p = place_of(k)
            part = pl.ds(pl.multiple_of(p * units, units), units)
            acc_c[...] += jnp.dot(
                hidden[p, group_rows(g)], w_down[part, :], preferred_element_type=f32
            )
            return 0

        with jax.named_scope("down"):
            lax.fori_loop(0, n_tp, body, 0)
        result[group_rows(g)] = acc_c[...].astype(bf16)
        others(g, lambda p: give_back(p, s).start())

    def relay_rows(g):
        with jax.named_scope("relay_rows"):
            relay(arrived, arrived_sems, g)

    def relay_hidden(g):
        with jax.named_scope("relay_hidden"):
            relay(hidden, hidden_sems, g)

    mix[...] = jnp.zeros_like(mix)
    choose()
    with jax.named_scope("right"):
        serve_right(1)
    with jax.named_scope("proj1"):
        for h in range(2):
            for i in range(2):
                project(z * 2 + i, h)
            project_chips(1, h)

    def project_far(j, _):
        for h in range(2):
            if h == 0:
                for i in range(2):
                    serve(j, 0, i)
            else:
                serve_right(j)
            project_chips(j, h)
        return 0

    lax.fori_loop(2, reach, project_far, 0)
    far_pair(near_low, -2, lambda shift: ask(shift).wait_recv())
    far_pair(near_high, 2, lambda shift: ask(shift).wait_recv())
    for h in range(2):
        with jax.named_scope("far"):
            for i in range(2):
                serve(reach, h, i)
            project_chips(reach, h)
        far_pair(near_low, -2, lambda shift, h=h: project_edge(shift, h))
        far_pair(near_high, 2, lambda shift, h=h: project_edge(shift, h))
    with jax.named_scope("edge"):
        far_pair(at_low, 2, add_edge)
        far_pair(at_high, -2, add_edge)
    with jax.named_scope("finish"):
        finish_rows()
    dispatch_to(quarter)
    dispatch_stage(-2)
    forward(0)
    with jax.named_scope("scale"):
        finish_scale()
    for load in loads:
        load.wait()
    dispatch_stage(-1)

    def early_sends():
        @pl.when(s < n_sp - 1)
        def _():
            def gone(c, _):
                hop(c).wait_send()
                return 0

            lax.fori_loop(0, total_pieces, gone, 0)

        for g in range(2):

            def heads_gone(k, _, g=g):
                heads_copy(g, k, t).wait_send()
                return 0

            lax.fori_loop(1, n_tp, heads_gone, 0)

        def passed(j, _):
            chip = chip_behind(j)

            @pl.when((chip >= 0) & (chip < chips))
            def _():
                for i in range(2):
                    b = chip * 2 + i

                    @pl.when(has_ahead & (j < reach))
                    def _():
                        @pl.when(j == 0)
                        def _():
                            along_line(b, 0).wait_send()

                        along_line(b, 1).wait_send()

                    @pl.when((b == s) | (j > 0))
                    def _():
                        for h in range(2):
                            to_partner(b, h).wait_send()

            return 0

        lax.fori_loop(0, reach + 1, passed, 0)
        far_pair(at_low, 2, lambda shift: ask(shift).wait_send())
        far_pair(at_high, -2, lambda shift: ask(shift).wait_send())
        for h in range(2):
            far_pair(near_low, -2, lambda shift, h=h: answer(shift, h).wait_send())
            far_pair(near_high, 2, lambda shift, h=h: answer(shift, h).wait_send())

    for step in range(GROUPS):
        if step > 0:
            dispatch_stage(step)
            forward(step)
            relay_rows(step - 1)
        if step >= 2:
            through_units(step - 2)
        if step >= 3:
            relay_hidden(step - 3)
        if step == 3:
            early_sends()
        if step >= 4:
            through_down(step - 4)
            finish_sends(arrived, arrived_sems, step - 4)
    last = GROUPS - 1
    relay_rows(last)
    through_units(last - 1)
    through_down(last - 3)
    relay_hidden(last - 2)
    through_units(last)
    through_down(last - 2)
    relay_hidden(last - 1)
    through_down(last - 1)
    relay_hidden(last)
    through_down(last)
    for g in range(GROUPS):
        others(g, lambda p: dispatch(p, s).wait_send())
        others(g, lambda p: scale_copy(p, s).wait_send())
        if g >= last - 3:
            finish_sends(arrived, arrived_sems, g)
        finish_sends(hidden, hidden_sems, g)

    returned[rows_of(s)] = result[rows_of(s)]
    with jax.named_scope("back"):
        for g in range(GROUPS):
            others(g, lambda p: give_back(p, p).wait_recv())
    combine_scope = jax.named_scope("combine")
    combine_scope.__enter__()
    total = stream_ref[...]
    for c in range(2):
        pick = jnp.dot(picks[c], returned[...], preferred_element_type=f32)
        total = total + shares[c][:, 0:1] * pick
    out_ref[...] = total.astype(bf16)
    combine_scope.__exit__(None, None, None)

    with jax.named_scope("sent"):
        for g in range(GROUPS):
            others(g, lambda p: give_back(p, s).wait_send())


def tables(rows, blocks, size):
    half = size // 2
    inverse = np.power(THETA, -np.arange(half) * 2.0 / size)
    inverse = np.concatenate([inverse, inverse])
    sign = np.where(np.arange(size) < half, -1.0, 1.0)

    def at(positions):
        angles = positions[:, None] * inverse[None, :]
        return jnp.asarray(np.stack([np.cos(angles), np.sin(angles) * sign]), jnp.float32)

    return at(np.arange(rows)), at(np.arange(blocks) * rows)


def per_device(
    residual,
    query_small,
    key_narrow_group,
    query_large,
    key_large,
    values,
    gates,
    log_decay,
    head_gain,
    out_weight,
    norm_gain,
    routes,
    route_weight,
    expert_gate,
    expert_up,
    expert_down,
):
    n_sp, n_tp = lax.axis_size("sp"), lax.axis_size("tp")
    row_count, cols = residual.shape
    head_count = log_decay.shape[2]
    bf16, f32 = jnp.bfloat16, jnp.float32
    size_a, size_b = query_small.shape[1] // head_count, query_large.shape[1] // head_count
    turn_a, start_a = tables(row_count, n_sp, size_a)
    turn_b, start_b = tables(row_count, n_sp, size_b)
    slots = 4 * row_count
    pieces = head_count * (1 + size_b // size_a)
    value_size = values.shape[2] // head_count
    width, units = expert_gate.shape[1:]
    dma = pltpu.SemaphoreType.DMA
    across, down = grid_of(n_tp)
    straights, relays = across + down - 2, (across - 1) * (down - 1)
    vmem = pl.BlockSpec(memory_space=pltpu.VMEM)
    hbm = pl.BlockSpec(memory_space=pl.ANY)
    inputs = (
        residual,
        query_small,
        key_narrow_group,
        query_large,
        key_large,
        values,
        gates,
        turn_a,
        start_a,
        turn_b,
        start_b,
        jnp.transpose(log_decay, (1, 2, 0)).reshape(2 * head_count, row_count),
        head_gain,
        norm_gain[None, :],
        routes.T,
        route_weight.T,
    )
    return pl.pallas_call(
        layer_kernel,
        out_shape=jax.ShapeDtypeStruct((row_count, cols), bf16),
        in_specs=[hbm] * (STAGED + 4),
        out_specs=vmem,
        scratch_shapes=[pltpu.VMEM(a.shape, a.dtype) for a in inputs]
        + [
            dma((STAGED,)),
            pltpu.VMEM((2, row_count, slots), bf16),
            pltpu.VMEM((slots, row_count), bf16),
            pltpu.VMEM((2, row_count, row_count), f32),
            pltpu.VMEM((row_count, cols), f32),
            pltpu.VMEM((row_count, 2 * head_count), f32),
            pltpu.VMEM((2 * head_count, row_count), f32),
            pltpu.VMEM(query_small.shape, bf16),
            pltpu.VMEM(query_large.shape, bf16),
            pltpu.VMEM((2 * head_count, row_count, value_size), f32),
            pltpu.VMEM((pieces, size_a, value_size), f32),
            pltpu.VMEM((pieces, 1, value_size), f32),
            pltpu.VMEM((pieces, size_a, value_size), bf16),
            pltpu.VMEM((pieces, size_a, value_size), bf16),
            pltpu.VMEM((n_tp, 2, row_count, values.shape[2]), bf16),
            pltpu.VMEM((n_sp,) + out_weight.shape, bf16),
            pltpu.VMEM((row_count, cols), f32),
            pltpu.VMEM((width, units), bf16),
            pltpu.VMEM((width, units), bf16),
            pltpu.VMEM(expert_down.shape[1:], bf16),
            pltpu.VMEM((n_tp, 8, row_count), f32),
            pltpu.VMEM((slots, cols), bf16),
            pltpu.VMEM((n_tp, slots, cols), bf16),
            pltpu.VMEM((n_tp, slots, units), bf16),
            pltpu.VMEM((slots, 128), bf16),
            pltpu.VMEM((slots, 128), bf16),
            pltpu.VMEM((2, row_count, values.shape[2]), bf16),
            pltpu.VMEM((row_count, cols), bf16),
            pltpu.VMEM((row_count, cols), bf16),
            pltpu.VMEM((slots, cols), bf16),
            pltpu.VMEM((slots, cols), bf16),
            pltpu.VMEM((slots // GROUPS, units), f32),
            pltpu.VMEM((slots // GROUPS, units), f32),
            pltpu.VMEM((slots // GROUPS, cols), f32),
            dma((4,)),
            dma((pieces,)),
            dma((pieces,)),
            dma((2, n_tp)),
            dma((2, n_tp)),
            dma((2, n_sp)),
            dma((2, n_sp)),
            dma((2, n_sp)),
            dma((3,)),
            dma((3,)),
            dma((n_tp,)),
            dma((n_tp,)),
            dma((n_sp,)),
            dma((n_sp,)),
            dma((n_sp,)),
            dma((n_sp,)),
            dma((GROUPS, straights)),
            dma((GROUPS, straights)),
            dma((GROUPS, 2, relays)),
            dma((GROUPS, 2, relays)),
            dma((GROUPS, straights)),
            dma((GROUPS, straights)),
            dma((GROUPS, 2, relays)),
            dma((GROUPS, 2, relays)),
            dma((n_sp,)),
            dma((n_sp,)),
        ],
        compiler_params=pltpu.CompilerParams(
            collective_id=0, has_side_effects=True, vmem_limit_bytes=58 * 2**20
        ),
    )(*inputs, out_weight, expert_gate, expert_up, expert_down)


def solution(mesh):
    placed = (
        P("sp", "tp"),
        P("sp", "tp"),
        P("sp", "tp"),
        P("sp", "tp"),
        P("sp", "tp"),
        P("sp", None, "tp"),
        P("sp", None, "tp"),
        P("sp", None, "tp"),
        P(None, "tp"),
        P(None, "sp", "tp"),
        P("tp"),
        P("sp", None),
        P("sp", None),
        P("sp", None, "tp"),
        P("sp", None, "tp"),
        P("sp", None, "tp"),
    )
    return jax.shard_map(
        per_device, mesh=mesh, in_specs=placed, out_specs=P("sp", "tp"), check_vma=False
    )
```
